32 devices in a mesh: ep: 8 (over z, x), tp: 4 (over y, core).
Axes of the slice: x: 2, y: 2, z: 4, core: 2. Of those that a mesh axis runs over, the one named last changes fastest.
Arguments:
- tokens: bfloat16 [384, 2048], P('ep'), may hold values from -6 to 6
- state: float32 [384, 8, 128, 128], P('ep', 'tp'), may hold values from -4 to 4
- norm_gain: float32 [2048], replicated, may hold values from 0.1 to 1.9
- w_query: bfloat16 [2048, 1024], P('ep', 'tp'), may hold values from -0.125 to 0.125
- w_forget: bfloat16 [2048, 1024], P('ep', 'tp'), may hold values from -0.125 to 0.125
- w_input: bfloat16 [2048, 1024], P('ep', 'tp'), may hold values from -0.125 to 0.125
- w_outgate: bfloat16 [2048, 1024], P('ep', 'tp'), may hold values from -0.125 to 0.125
- lower_bound: float32 [1024], P('tp'), may hold values from 0 to 0.9
- head_gain: float32 [1024], P('tp'), may hold values from 0.1 to 1.9
- w_output: bfloat16 [1024, 2048], P('tp'), may hold values from -0.1875 to 0.1875
- ffn_gain: float32 [2048], replicated, may hold values from 0.1 to 1.9
- route_ids: int32 [384, 4], P('ep'), may hold values from 0 to 15, all different within a row; in each aligned block of 48 rows (0 to 47, 48 to 95, ...) at most 24 rows name the same one
- route_weight: float32 [384, 4], P('ep'), may hold values from 0.2 to 1
- expert_gate: bfloat16 [16, 2048, 1024], P('ep', None, 'tp'), may hold values from -0.125 to 0.125
- expert_up: bfloat16 [16, 2048, 1024], P('ep', None, 'tp'), may hold values from -0.125 to 0.125
- expert_down: bfloat16 [16, 1024, 2048], P('ep', 'tp'), may hold values from -0.1875 to 0.1875
- shared_gate: bfloat16 [2048, 1024], P(None, 'tp'), may hold values from -0.125 to 0.125
- shared_up: bfloat16 [2048, 1024], P(None, 'tp'), may hold values from -0.125 to 0.125
- shared_down: bfloat16 [1024, 2048], P('tp'), may hold values from -0.1875 to 0.1875
- dense_gate: bfloat16 [2048, 8192], P('tp', 'ep'), may hold values from -0.125 to 0.125
- dense_up: bfloat16 [2048, 8192], P('tp', 'ep'), may hold values from -0.125 to 0.125
- dense_down: bfloat16 [8192, 2048], P('ep', 'tp'), may hold values from -0.0625 to 0.0625
- dense_mix: float32 [2048], P('tp'), may hold values from -6 to 6
Outputs:
- mixed: bfloat16 [384, 2048], P('ep', 'tp')
- new_state: float32 [384, 8, 128, 128], P('ep', 'tp')
The draws below stay inside these ranges and needn't reach their ends.
Inputs may be any that keep to these rules, and one draw needn't show every extreme that they name: `route_ids`: each row names 4 different experts. Among the rows of one device no expert is named more than 24 times, and in every draw some expert is named exactly 24 times by some device's rows.
All inputs are finite; a program needn't handle non-finite values.
Results may differ from the reference program's by a relative error of at most 0.025.
Values may be sent and summed in bfloat16 or wider, within the bound.
A program may use at most 64 MiB of HBM per device.

```python
import math
import jax
import jax.numpy as jnp
import numpy as np
from jax import lax

WIDTH = 2048
HEADS = 8
HEAD_DIM = 128
MIX_WIDTH = 1024
EXPERTS = 16
TOPK = 4
EXPERT_FF = 1024
SHARED_FF = 1024
DENSE_FF = 8192
SEQ_DEV = 48
BATCH = 384
CAP = 24
N_EP = 8
N_TP = 4


def shard_levels(rng, extent, cuts, smallest, largest):
    level = 1.0
    for axis_at, blocks in cuts:
        steps = jax.random.uniform(jax.random.fold_in(jax.random.fold_in(rng, 6), axis_at), (blocks,), jnp.float32, smallest / len(cuts), largest / len(cuts))
        level = level * jnp.repeat(jnp.exp(steps), extent[axis_at] // blocks).reshape((-1,) + (1,) * (len(extent) - 1 - axis_at))
    return level


def assign_block(key, own, number, rows, amount, top, limit, skew):
    order = jax.random.permutation(key, amount)
    crowded, usual = portions_of(amount, rows * top, limit, skew, True), portions_of(amount, rows * top, limit, skew, False)
    places = jnp.arange(amount)

    def named(tallies, turn):
        used = int((tallies > 0).sum())
        fixed = max(1, used // 4)
        moved = fixed + (places - fixed + turn * (used - fixed)) % max(1, amount - fixed)
        return jnp.zeros((amount,), jnp.int32).at[order[jnp.where(places < fixed, places, moved)]].set(jnp.asarray(tallies, jnp.int32))

    tallies = jnp.where(number % 4 == 0, named(crowded, number // 4), named(usual, number - number // 4 - 1))
    mixed = jax.random.permutation(jax.random.fold_in(own, 3), amount)
    giver, taker = mixed[0:amount // 2 * 2:2], mixed[1:amount // 2 * 2:2]
    room = jnp.minimum(tallies[giver] - 1, limit - tallies[taker]) // 2
    room = jnp.where((giver == order[0]) | (taker == order[0]) | (tallies[taker] == 0), 0, jnp.maximum(room, 0))
    moved = jax.random.randint(jax.random.fold_in(own, 4), (amount // 2,), 0, 1 << 20) % (room + 1)
    tallies = tallies.at[giver].add(-moved).at[taker].add(moved)
    members = jnp.searchsorted(jnp.cumsum(tallies), jnp.arange(rows * top), side="right").astype(jnp.int32)
    listing = members.reshape(top, rows).T
    listing = listing[jax.random.permutation(jax.random.fold_in(own, 1), rows)]
    turn = jax.random.randint(jax.random.fold_in(own, 2), (rows, 1), 0, top)
    return jnp.take_along_axis(listing, (jnp.arange(top)[None, :] + turn) % top, axis=1)


def portions_of(count, total, reach, skew, full):
    loads = [(1 << 20) // math.isqrt(rank ** skew) + 1 for rank in range(1, count + 1)]
    largest = reach if full else min(reach, max(-(-total // count), total * loads[0] // sum(loads)))
    least = 1 if total - largest >= count - 1 else 0
    holding, rest = [largest] + [least] * (count - 1), total - largest - least * (count - 1)
    while rest > 0:
        movable = [i for i in range(1, count) if holding[i] < largest] or [i for i in range(1, count) if holding[i] < reach]
        whole, remaining = sum([loads[i] for i in movable]), rest
        for i in movable:
            more = min(reach - holding[i], max(1, remaining * loads[i] // whole), rest)
            holding[i] = holding[i] + more
            rest = rest - more
    return np.array(holding)


def bell_draw(stream_key, shape, deviation, bound, cuts=(), held_as=jnp.bfloat16):
    result = deviation * jax.random.normal(stream_key, shape, jnp.float32)
    if cuts:
        result = result * shard_levels(stream_key, shape, cuts, -0.22, 0.18)
    return jnp.clip(result, -bound, bound).astype(held_as)


def setup_inputs(seed: int = 0) -> dict:
    keys = jax.random.split(jax.random.key(seed), 24)
    tokens = bell_draw(keys[0], (BATCH, WIDTH), 1.0, 6.0, ((0, 8),))
    state = bell_draw(keys[1], (BATCH, HEADS, HEAD_DIM, HEAD_DIM), 0.5, 4.0, ((0, 8), (1, 4)), jnp.float32)
    norm_gain = jnp.clip(1.0 + 0.18 * jax.random.normal(keys[2], (WIDTH,), jnp.float32), 0.1, 1.9)
    w_query = bell_draw(keys[3], (WIDTH, MIX_WIDTH), WIDTH ** -0.5, 0.125, ((0, 8), (1, 4)))
    w_forget = bell_draw(keys[4], (WIDTH, MIX_WIDTH), WIDTH ** -0.5, 0.125, ((0, 8), (1, 4)))
    w_input = bell_draw(keys[5], (WIDTH, MIX_WIDTH), WIDTH ** -0.5, 0.125, ((0, 8), (1, 4)))
    w_outgate = bell_draw(keys[6], (WIDTH, MIX_WIDTH), WIDTH ** -0.5, 0.125, ((0, 8), (1, 4)))
    lower_bound = jnp.clip(0.9 * jax.random.uniform(keys[7], (MIX_WIDTH,), jnp.float32) ** shard_levels(keys[7], (MIX_WIDTH,), ((0, 4),), -0.2, 0.2), 0.0, 0.9)
    head_gain = jnp.clip(1.0 + 0.18 * jax.random.normal(keys[8], (MIX_WIDTH,), jnp.float32), 0.1, 1.9)
    w_output = bell_draw(keys[9], (MIX_WIDTH, WIDTH), MIX_WIDTH ** -0.5, 0.1875, ((0, 4),))
    ffn_gain = jnp.clip(1.0 + 0.18 * jax.random.normal(keys[10], (WIDTH,), jnp.float32), 0.1, 1.9)
    route_ids_keys = jax.random.split(jax.random.fold_in(keys[11], 1), BATCH // SEQ_DEV)
    route_ids_turns = jax.random.permutation(jax.random.fold_in(keys[11], 3), BATCH // SEQ_DEV)
    route_ids = jax.vmap(lambda own, number: assign_block(jax.random.fold_in(keys[11], 2), own, number, SEQ_DEV, EXPERTS, TOPK, CAP, 2))(route_ids_keys, route_ids_turns).reshape((BATCH, TOPK))
    route_weight = jnp.clip(0.2 + 0.8 * jax.random.uniform(keys[12], (BATCH, TOPK), jnp.float32) ** shard_levels(keys[12], (BATCH, TOPK), ((0, 8),), -0.2, 0.2), 0.2, 1.0)
    expert_gate = bell_draw(keys[13], (EXPERTS, WIDTH, EXPERT_FF), WIDTH ** -0.5, 0.125, ((0, 8), (2, 4)))
    expert_up = bell_draw(keys[14], (EXPERTS, WIDTH, EXPERT_FF), WIDTH ** -0.5, 0.125, ((0, 8), (2, 4)))
    expert_down = bell_draw(keys[15], (EXPERTS, EXPERT_FF, WIDTH), EXPERT_FF ** -0.5, 0.1875, ((0, 8), (1, 4)))
    shared_gate = bell_draw(keys[16], (WIDTH, SHARED_FF), WIDTH ** -0.5, 0.125, ((1, 4),))
    shared_up = bell_draw(keys[17], (WIDTH, SHARED_FF), WIDTH ** -0.5, 0.125, ((1, 4),))
    shared_down = bell_draw(keys[18], (SHARED_FF, WIDTH), SHARED_FF ** -0.5, 0.1875, ((0, 4),))
    dense_gate = bell_draw(keys[19], (WIDTH, DENSE_FF), WIDTH ** -0.5, 0.125, ((0, 4), (1, 8)))
    dense_up = bell_draw(keys[20], (WIDTH, DENSE_FF), WIDTH ** -0.5, 0.125, ((0, 4), (1, 8)))
    dense_down = bell_draw(keys[21], (DENSE_FF, WIDTH), DENSE_FF ** -0.5, 0.0625, ((0, 8), (1, 4)))
    dense_mix = bell_draw(keys[22], (WIDTH,), 1.5, 6.0, ((0, 4),), jnp.float32)
    return dict(tokens=tokens, state=state, norm_gain=norm_gain, w_query=w_query, w_forget=w_forget, w_input=w_input, w_outgate=w_outgate, lower_bound=lower_bound, head_gain=head_gain, w_output=w_output, ffn_gain=ffn_gain, route_ids=route_ids, route_weight=route_weight, expert_gate=expert_gate, expert_up=expert_up, expert_down=expert_down, shared_gate=shared_gate, shared_up=shared_up, shared_down=shared_down, dense_gate=dense_gate, dense_up=dense_up, dense_down=dense_down, dense_mix=dense_mix)


EPS = 1e-06

def rms_scale(values, gain):
    values = values.astype(jnp.float32)
    return values * lax.rsqrt(lax.optimization_barrier(jnp.mean(values * values, axis=-1, keepdims=True)) + EPS) * gain

def rounded(values):
    return lax.optimization_barrier(values.astype(jnp.bfloat16)).astype(jnp.float32)

def blocked_sum(left, right, pieces):
    inner = left.shape[1] // pieces
    total = jnp.zeros((left.shape[0], right.shape[1]), jnp.float32)
    for index in range(pieces):
        part = jnp.dot(left[:, index * inner:(index + 1) * inner], right[index * inner:(index + 1) * inner], preferred_element_type=jnp.float32)
        total = total + rounded(part)
    return total

def reference(tokens, state, norm_gain, w_query, w_forget, w_input, w_outgate, lower_bound, head_gain, w_output, ffn_gain, route_ids, route_weight, expert_gate, expert_up, expert_down, shared_gate, shared_up, shared_down, dense_gate, dense_up, dense_down, dense_mix):
    batch = tokens.shape[0]
    normed = rms_scale(tokens, norm_gain).astype(jnp.bfloat16)

    def project(weight):
        return rounded(jnp.dot(normed, weight, preferred_element_type=jnp.float32))
    query, forget_pre, values, out_gate = [project(w) for w in (w_query, w_forget, w_input, w_outgate)]
    forget_sig = jax.nn.sigmoid(forget_pre)
    shape = (batch, HEADS, HEAD_DIM)
    decay = (lower_bound + (1.0 - lower_bound) * forget_sig).reshape(shape)
    keygate = ((1.0 - lower_bound) * (1.0 - forget_sig)).reshape(shape)
    new_state = decay[..., None] * state + keygate[..., None] * values.reshape(shape)[:, :, None, :]
    readout = jnp.einsum('bhk,bhkv->bhv', query.reshape(shape), new_state, precision=lax.Precision.HIGHEST)
    readout = readout * lax.rsqrt(lax.optimization_barrier(jnp.mean(readout * readout, axis=-1, keepdims=True)) + EPS)
    head_out = (readout.reshape(batch, MIX_WIDTH) * head_gain * jax.nn.silu(out_gate)).astype(jnp.bfloat16)
    resid = tokens.astype(jnp.float32) + blocked_sum(head_out, w_output, N_TP)
    moe_in = rms_scale(resid, ffn_gain).astype(jnp.bfloat16)
    flat_ids = route_ids.reshape(N_EP, SEQ_DEV * TOPK)
    onehot = (flat_ids[..., None] == jnp.arange(EXPERTS, dtype=jnp.int32)).astype(jnp.int32)
    slot_rank = lax.optimization_barrier(jnp.sum((jnp.cumsum(onehot, axis=1) - onehot) * onehot, axis=-1))
    device = jnp.arange(N_EP, dtype=jnp.int32)[:, None]
    slot_index = ((flat_ids * N_EP + device) * CAP + slot_rank).reshape(-1).astype(jnp.int32)
    token_index = jnp.repeat(jnp.arange(batch, dtype=jnp.int32), TOPK)
    table = jnp.full((EXPERTS * N_EP * CAP,), batch, jnp.int32).at[slot_index].set(token_index)
    padded = jnp.concatenate([moe_in, jnp.zeros((1, WIDTH), jnp.bfloat16)], axis=0)
    gathered = padded[table].reshape(EXPERTS, N_EP * CAP, WIDTH)

    def one_expert(args):
        rows_in, gate_weight, up_weight, down_weight = args
        gate_pre = jnp.dot(rows_in, gate_weight, preferred_element_type=jnp.float32)
        up_pre = jnp.dot(rows_in, up_weight, preferred_element_type=jnp.float32)
        hidden = (jax.nn.silu(gate_pre) * up_pre).astype(jnp.bfloat16)
        return blocked_sum(hidden, down_weight, N_TP).astype(jnp.bfloat16)
    outputs = lax.map(one_expert, (gathered, expert_gate, expert_up, expert_down)).reshape(-1, WIDTH)
    picked = outputs[slot_index].reshape(batch, TOPK, WIDTH).astype(jnp.float32)
    routed = lax.optimization_barrier(jnp.sum(route_weight[..., None] * picked, axis=1))
    shared_hidden = (jax.nn.silu(jnp.dot(moe_in, shared_gate, preferred_element_type=jnp.float32)) * jnp.dot(moe_in, shared_up, preferred_element_type=jnp.float32)).astype(jnp.bfloat16)
    shared_out = blocked_sum(shared_hidden, shared_down, N_TP)
    dense_pre_gate = blocked_sum(moe_in, dense_gate, N_TP)
    dense_pre_up = blocked_sum(moe_in, dense_up, N_TP)
    dense_hidden = (jax.nn.silu(dense_pre_gate) * dense_pre_up).astype(jnp.bfloat16)
    dense_out = jnp.dot(dense_hidden, dense_down, preferred_element_type=jnp.float32)
    mixed = (resid + routed + shared_out + jax.nn.sigmoid(dense_mix) * dense_out).astype(jnp.bfloat16)
    return (mixed, new_state)
```

```python
import functools
import types

import jax
import jax.numpy as jnp
from jax import lax
from jax.experimental import pallas as pl
from jax.experimental.pallas import tpu as pltpu
from jax.sharding import PartitionSpec as P

EPS = 1e-06
LANES = 128
CORES = 2
ROWS = 8
F32 = jnp.float32
BF16 = jnp.bfloat16
VMEM_BYTES = 60 * 1024 * 1024
(
    WEIGHT,
    NORMED,
    MOVE,
    ROUTE,
    MIX,
    PROJ,
    HEAD,
    GATHER_Z,
    GATHER_A,
    GATHER_B,
    GATHER_C,
    SQUARE,
    SCALE,
    SUM_C,
    SUM_A,
    SUM_B,
    SUM_Z,
) = range(17)


def span(index, size):
    if isinstance(index, int):
        return pl.ds(index * size, size)
    return pl.ds(pl.multiple_of(index * size, size), size)


def ceil_to(value, step):
    return -(-value // step) * step


def silu(v):
    return v * jax.nn.sigmoid(v)


def layer_kernel(n, tpn, move, names, *refs):
    sems = refs[len(names) :]
    r = types.SimpleNamespace(**dict(zip(names, refs)))
    me, tp = lax.axis_index("ep"), lax.axis_index("tp")
    sides = tpn // CORES
    xs = sides
    zs = n // xs
    z, x = lax.div(me, xs), lax.rem(me, xs)
    y, c = lax.div(tp, CORES), lax.rem(tp, CORES)
    twin_core = CORES - 1 - c
    seq, width = r.tokens.shape
    cols = width // tpn
    depth, mixw = r.wq.shape
    exp_local, _, ff = r.eg.shape
    sff = r.sg.shape[1]
    dff = r.dgv.shape[2]
    heads, hd = r.state.shape[1:3]
    wrap = xs * depth
    lanes = r.scs.shape[1]
    half = sides * cols

    def pick(first, second):
        return first * (1 - c) + second * c

    def device(zz, xx, yy, cc):
        return {"ep": zz * xs + xx, "tp": yy * CORES + cc}

    waiting = []

    def send(src, dst, kind, slot, peer):
        copy = pltpu.make_async_remote_copy(
            src_ref=src,
            dst_ref=dst,
            send_sem=sems[2 * kind].at[slot],
            recv_sem=sems[2 * kind + 1].at[slot],
            device_id=peer,
            device_id_type=pl.DeviceIdType.MESH,
        )
        copy.start()
        waiting.append(copy)
        return copy

    used = [0]

    def fetch(src, dst):
        copy = pltpu.make_async_copy(src, dst, r.local.at[used[0]])
        used[0] += 1
        copy.start()
        return copy

    got = types.SimpleNamespace()
    got.tokens = fetch(r.tokens, r.tokens_v)
    got.gain1 = fetch(r.gain1, r.gain1_v)
    order = (r.wf, r.wq, r.wi, r.wo)
    got.w = [fetch(w, r.wbuf.at[i, span(x, depth), :]) for i, w in enumerate(order)]
    got.lb = fetch(r.lb, r.lb_v)
    got.hg = fetch(r.hg, r.hg_v)
    got.mix = fetch(r.mix, r.mix_v)
    got.ids = fetch(r.ids, r.ids_v)
    got.weights = fetch(r.weights, r.weights_v)
    groups = seq // ROWS
    states = [
        fetch(r.state.at[pl.ds(g * ROWS, ROWS)], r.st.at[pl.ds(g * ROWS, ROWS)])
        for g in range(groups)
    ]
    got.wout = fetch(r.wout, r.wout_v)
    got.gain2 = fetch(r.gain2, r.gain2_v)

    barrier = pltpu.get_barrier_semaphore()
    for s in range(1, tpn):
        pl.semaphore_signal(
            barrier,
            inc=1,
            device_id={"tp": lax.rem(tp + s, tpn)},
            device_id_type=pl.DeviceIdType.MESH,
        )
    for s in range(1, n):
        pl.semaphore_signal(
            barrier,
            inc=1,
            device_id={"ep": lax.rem(me + s, n)},
            device_id_type=pl.DeviceIdType.MESH,
        )
    got.tokens.wait()
    got.gain1.wait()
    t32 = r.tokens_v[...].astype(F32)
    normed = (
        t32 * lax.rsqrt(jnp.mean(t32 * t32, axis=-1, keepdims=True) + EPS) * r.gain1_v[...]
    ).astype(BF16)
    for d in range(zs):
        r.nsend[d * seq : (d + 1) * seq, :] = normed[:, d * wrap : (d + 1) * wrap]
    r.ncol[span(z, seq), :] = r.nsend[span(z, seq), :]
    pl.semaphore_wait(barrier, n - 1 + tpn - 1)

    arrived = {}
    for i, w in enumerate(order):
        for s in range(1, xs):
            arrived[WEIGHT, i, s] = send(
                w,
                r.wbuf.at[i, span(x, depth), :],
                WEIGHT,
                i * xs + s,
                device(z, lax.rem(x + s, xs), y, c),
            )
    for s in range(1, zs):
        zz = lax.rem(z + s, zs)
        arrived[NORMED, s] = send(
            r.nsend.at[span(zz, seq)],
            r.ncol.at[span(z, seq)],
            NORMED,
            s,
            device(zz, x, y, c),
        )
    if move:
        got.dgv = []
        for i, (src, dst) in enumerate(((r.dgate, r.dgv), (r.dup, r.duv))):
            rows = src.shape[0]
            for s in range(1, tpn):
                peer = lax.rem(tp + s, tpn)
                arrived[MOVE, i, s] = send(
                    src.at[:, span(peer, dff)],
                    dst.at[c, span(y, rows), :],
                    MOVE,
                    i * tpn + s,
                    {"tp": peer},
                )
            got.dgv.append(fetch(src.at[:, span(tp, dff)], dst.at[c, span(y, rows), :]))

    got.ids.wait()
    got.weights.wait()
    got.mix.wait()
    eye = lax.broadcasted_iota(jnp.int32, (seq, lanes), 0) == lax.broadcasted_iota(
        jnp.int32, (seq, lanes), 1
    )
    ids, weights = r.ids_v[...], r.weights_v[...]
    rrows = r.rsend.shape[1]

    def to_row(col):
        return jnp.sum(jnp.where(eye, col, 0.0), axis=0, keepdims=True)

    def to_col(row):
        return jnp.sum(jnp.where(eye, row, 0.0), axis=1, keepdims=True)

    for d in range(n):
        r.rsend[d] = jnp.zeros((rrows, lanes), F32)
        for i in range(exp_local):
            r.rsend[d, i : i + 1, :seq] = jnp.sum(
                jnp.where(ids == d * exp_local + i, weights, 0.0), axis=0, keepdims=True
            )
    r.rrecv[me] = r.rsend[me]
    for s in range(1, n):
        peer = lax.rem(me + s, n)
        arrived[ROUTE, s] = send(
            r.rsend.at[peer], r.rrecv.at[me], ROUTE, s, {"ep": peer}
        )
    r.mixs[...] = jnp.broadcast_to(jax.nn.sigmoid(r.mix_v[...]), (ROWS, cols))
    r.mixr[tp] = r.mixs[...]
    for s in range(1, tpn):
        arrived[MIX, s] = send(
            r.mixs, r.mixr.at[tp], MIX, s, {"tp": lax.rem(tp + s, tpn)}
        )

    def fetch_rows(src, dst):
        return [
            fetch(src.at[span(t, cols), :], dst(t % CORES).at[span(t // CORES, cols), :])
            for t in range(tpn)
        ]

    got.sgv = fetch_rows(r.sg, lambda k: r.sgv.at[k]) + fetch_rows(r.su, lambda k: r.suv.at[k])
    got.sdv = [fetch(r.sd, r.sdv)]
    got.egv = []
    for e in range(exp_local):
        got.egv += fetch_rows(r.eg.at[e], lambda k: r.egv.at[k, e])
        got.egv += fetch_rows(r.eu.at[e], lambda k: r.euv.at[k, e])
    got.edv = [fetch(r.ed.at[e], r.edv.at[span(e, ff), :]) for e in range(exp_local)]
    if move:
        got.ddv = [fetch(r.ddown.at[span(tp, dff), :], r.ddv.at[tp])]
    else:
        got.dgv = fetch_rows(r.gatew, lambda k: r.dgv.at[k])
        got.dgv += fetch_rows(r.upw, lambda k: r.duv.at[k])
        got.ddv = [fetch(r.downw.at[:, span(t, cols)], r.ddv.at[t]) for t in range(tpn)]

    for s in range(1, zs):
        arrived[NORMED, s].wait_recv()
    for i in range(len(order)):
        got.w[i].wait()
        for s in range(1, xs):
            arrived[WEIGHT, i, s].wait_recv()
        r.psend[i] = jnp.dot(
            r.ncol[...], r.wbuf[i], preferred_element_type=F32
        ).astype(BF16)
        for s in range(1, zs):
            zz = lax.rem(z + s, zs)
            arrived[PROJ, i, s] = send(
                r.psend.at[i, span(zz, seq)],
                r.precv.at[i, span(z, seq)],
                PROJ,
                i * zs + s,
                device(zz, x, y, c),
            )

    def projected(i):
        total = r.psend[i, span(z, seq), :].astype(F32)
        for s in range(1, zs):
            arrived[PROJ, i, s].wait_recv()
            total = total + r.precv[i, span(lax.rem(z + zs - s, zs), seq), :].astype(F32)
        return total.astype(BF16).astype(F32)

    padded = ceil_to(seq, LANES)

    def turn(value, dst):
        if padded > seq:
            value = jnp.concatenate([value, jnp.zeros((padded - seq, mixw), F32)], axis=0)
        value = value.T
        for g in range(groups):
            dst[g] = value[:, g * ROWS : (g + 1) * ROWS]

    got.lb.wait()
    got.hg.wait()
    lb = r.lb_v[...]
    turn(lb + (1.0 - lb) * jax.nn.sigmoid(projected(0)), r.dturn)
    turn(projected(1), r.qturn)
    r.vals[...] = projected(2)
    for copy in states:
        copy.wait()

    def group(g, carry):
        dg, qg = r.dturn[g], r.qturn[g]
        vg = r.vals[span(g, ROWS), :]
        rows = []
        for b in range(ROWS):
            parts = []
            for h in range(heads):
                at = slice(h * hd, (h + 1) * hd)
                vrow = vg[b : b + 1, at]
                new = vrow + dg[at, b : b + 1] * (r.st[g * ROWS + b, h] - vrow)
                r.st[g * ROWS + b, h] = new
                parts.append(jnp.sum(qg[at, b : b + 1] * new, axis=0, keepdims=True))
            rows.append(jnp.concatenate(parts, axis=1))
        r.read[span(g, ROWS), :] = jnp.concatenate(rows, axis=0)
        pltpu.make_async_copy(
            r.st.at[span(g, ROWS)], r.new_state.at[span(g, ROWS)], r.stout.at[g]
        ).start()
        return carry

    lax.fori_loop(0, groups, group, 0)
    read = r.read[...]
    read = jnp.concatenate(
        [
            part * lax.rsqrt(jnp.mean(part * part, axis=-1, keepdims=True) + EPS)
            for part in [read[:, h * hd : (h + 1) * hd] for h in range(heads)]
        ],
        axis=1,
    )
    head = (read * r.hg_v[...] * silu(projected(3))).astype(BF16)

    got.wout.wait()
    got.gain2.wait()
    for t in range(tpn):
        r.hsend[t] = jnp.dot(
            head, r.wout_v[:, t * cols : (t + 1) * cols], preferred_element_type=F32
        ).astype(BF16)
    for s in range(1, tpn):
        peer = lax.rem(tp + s, tpn)
        arrived[HEAD, s] = send(r.hsend.at[peer], r.hrecv.at[tp], HEAD, s, {"tp": peer})
    mine = span(tp, cols)
    total = r.tokens_v[:, mine].astype(F32) + r.hsend[tp].astype(F32)
    for s in range(1, tpn):
        arrived[HEAD, s].wait_recv()
        total = total + r.hrecv[lax.rem(tp + tpn - s, tpn)].astype(F32)
    r.resid[...] = total

    def block(zz, xx, yy, cc):
        return r.rows.at[cc, span(zz * xs + xx, seq), span(yy, cols)]

    r.rows[c, span(me, seq), span(y, cols)] = (total * r.gain2_v[:, mine]).astype(BF16)
    own = block(z, x, y, c)
    for s in range(1, zs):
        arrived[GATHER_Z, s] = send(own, own, GATHER_Z, s, device(lax.rem(z + s, zs), x, y, c))

    def plane(s, a, b):
        zz = lax.rem(z + zs - s, zs)
        xx = lax.rem(x + xs - pick(a, b), xs)
        yy = lax.rem(y + sides - pick(b, a), sides)
        return block(zz, xx, yy, c)

    def forward_first(s):
        ref = plane(s, 0, 0)
        for q in range(1, sides):
            peer = device(z, lax.rem(x + pick(q, 0), xs), lax.rem(y + pick(0, q), sides), c)
            arrived[GATHER_A, s, q] = send(ref, ref, GATHER_A, s * sides + q, peer)

    def forward_second(s, a):
        ref = plane(s, a, 0)
        for q in range(1, sides):
            peer = device(z, lax.rem(x + pick(0, q), xs), lax.rem(y + pick(q, 0), sides), c)
            arrived[GATHER_B, s, a, q] = send(ref, ref, GATHER_B, (s * sides + a) * sides + q, peer)

    def forward_twin(s, a, b):
        ref = plane(s, a, b)
        arrived[GATHER_C, s, a, b] = send(
            ref, ref, GATHER_C, (s * sides + a) * sides + b, device(z, x, y, twin_core)
        )

    forward_first(0)
    forward_second(0, 0)
    forward_twin(0, 0, 0)

    square = to_row(jnp.sum(total * total, axis=-1, keepdims=True))
    r.sqs[...] = jnp.broadcast_to(square, (ROWS, lanes))
    for s in range(1, tpn):
        arrived[SQUARE, s] = send(
            r.sqs, r.sqr.at[tp], SQUARE, s, {"tp": lax.rem(tp + s, tpn)}
        )
    for s in range(1, tpn):
        arrived[SQUARE, s].wait_recv()
        square = square + r.sqr[lax.rem(tp + tpn - s, tpn)][:1]
    scale = lax.rsqrt(square / width + EPS)
    r.scs[...] = jnp.broadcast_to(scale, (ROWS, lanes))
    r.scr[me] = r.scs[...]
    for s in range(1, n):
        arrived[SCALE, s] = send(r.scs, r.scr.at[me], SCALE, s, {"ep": lax.rem(me + s, n)})

    for s in range(zs):
        if s:
            arrived[GATHER_Z, s].wait_recv()
            forward_first(s)
            forward_second(s, 0)
            forward_twin(s, 0, 0)
        for a in range(1, sides):
            arrived[GATHER_A, s, a].wait_recv()
            forward_second(s, a)
            forward_twin(s, a, 0)
    if move:
        for s in range(1, tpn):
            peer = lax.rem(tp + s, tpn)
            arrived[MOVE, 2, s] = send(
                r.ddown.at[span(peer, dff), :],
                r.ddv.at[tp],
                MOVE,
                2 * tpn + s,
                {"tp": peer},
            )
    for s in range(zs):
        for a in range(sides):
            for b in range(1, sides):
                arrived[GATHER_B, s, a, b].wait_recv()
                forward_twin(s, a, b)

    pairs = [(r.egv, r.euv, e) for e in range(exp_local)] + [(r.dgv, r.duv, None)]

    def weight(ref, lead, plane_at):
        return ref[plane_at] if lead is None else ref[plane_at, lead]

    for copy in got.egv:
        copy.wait()
    for k, (gate, up, lead) in enumerate(pairs):
        if lead is None:
            for copy in got.dgv:
                copy.wait()
            if move:
                for i in range(2):
                    for s in range(1, tpn):
                        arrived[MOVE, i, s].wait_recv()
        acc = r.acc if lead is not None else r.dacc
        base = 2 * k if lead is not None else 0
        for j, ref in enumerate((gate, up)):
            acc[base + j] = jnp.dot(
                r.rows[c], weight(ref, lead, c), preferred_element_type=F32
            )

    for s in range(zs):
        for a in range(sides):
            for b in range(sides):
                arrived[GATHER_C, s, a, b].wait_recv()

    for copy in got.sgv + got.sdv:
        copy.wait()
    for s in range(1, n):
        arrived[SCALE, s].wait_recv()
        arrived[ROUTE, s].wait_recv()
    for s in range(1, tpn):
        arrived[MIX, s].wait_recv()
    pre = []
    for ref in (r.sgv, r.suv):
        pre.append(
            sum(
                jnp.dot(r.rows[k, span(me, seq), :], ref[k], preferred_element_type=F32)
                for k in range(CORES)
            )
        )
    own_scale = to_col(scale)
    shared_hidden = (silu(own_scale * pre[0]) * (own_scale * pre[1])).astype(BF16)
    for t in range(tpn):
        r.shared[t] = jnp.dot(
            shared_hidden, r.sdv[:, t * cols : (t + 1) * cols], preferred_element_type=F32
        )

    scales = jnp.concatenate([to_col(r.scr[e][:1]) for e in range(n)], axis=0)
    for k, (gate, up, lead) in enumerate(pairs):
        acc = r.acc if lead is not None else r.dacc
        base = 2 * k if lead is not None else 0
        both = [
            scales
            * (
                acc[base + j]
                + jnp.dot(
                    r.rows[twin_core],
                    weight(ref, lead, twin_core),
                    preferred_element_type=F32,
                )
            )
            for j, ref in enumerate((gate, up))
        ]
        hidden = silu(both[0]) * both[1]
        if lead is None:
            r.dhid[...] = hidden.astype(BF16)
        else:
            share = jnp.concatenate(
                [to_col(r.rrecv[e][lead : lead + 1]) for e in range(n)], axis=0
            )
            r.hid[:, k * ff : (k + 1) * ff] = (hidden * share).astype(BF16)
    for copy in got.edv + got.ddv:
        copy.wait()
    if move:
        for s in range(1, tpn):
            arrived[MOVE, 2, s].wait_recv()

    def partial(t):
        routed = jnp.dot(
            r.hid[...], r.edv[:, span(t, cols)], preferred_element_type=F32
        )
        dense = jnp.dot(r.dhid[...], r.ddv[t], preferred_element_type=F32)
        return routed + r.mixr[t][:1] * dense

    for q in [*range(1, sides), 0]:
        yy = lax.rem(y + q, sides)
        t = yy * CORES + twin_core
        r.part[q] = partial(t).astype(BF16)
        r.part[q, span(me, seq), :] = (
            r.part[q, span(me, seq), :].astype(F32) + r.shared[t]
        ).astype(BF16)
        arrived[SUM_C, q] = send(
            r.part.at[q], r.crecv.at[q], SUM_C, q, device(z, x, y, twin_core)
        )
    for q in [*range(1, sides), 0]:
        yy = lax.rem(y + q, sides)
        t = yy * CORES + c
        mypart = partial(t)
        arrived[SUM_C, q].wait_recv()
        r.both[yy] = (mypart + r.crecv[q].astype(F32)).astype(BF16)
        r.both[yy, span(me, seq), :] = (
            r.both[yy, span(me, seq), :].astype(F32) + r.shared[t]
        ).astype(BF16)
    zorder = [*range(1, zs), 0]
    rorder = [*range(1, sides), 0]

    def summed(si, q, j):
        zz = lax.rem(z + si, zs)
        xx = lax.rem(x + pick(j, q), xs)
        yy = lax.rem(y + pick(q, j), sides)
        return r.both.at[yy, span(zz * xs + xx, seq), :]

    for si in zorder:
        for j in rorder:
            for q in range(1, sides):
                slot = (si * sides + j) * sides + q
                peer = device(
                    z, lax.rem(x + pick(0, q), xs), lax.rem(y + pick(q, 0), sides), c
                )
                arrived[SUM_A, si, j, q] = send(
                    summed(si, q, j), r.arecv.at[slot], SUM_A, slot, peer
                )

    def second(si):
        for j in rorder:
            value = summed(si, 0, j)[...].astype(F32)
            for q in range(1, sides):
                arrived[SUM_A, si, j, q].wait_recv()
                value = value + r.arecv[(si * sides + j) * sides + q].astype(F32)
            if j == 0:
                r.keep[si] = value
                continue
            slot = si * sides + j
            r.bsend[slot] = value.astype(BF16)
            peer = device(z, lax.rem(x + pick(j, 0), xs), lax.rem(y + pick(0, j), sides), c)
            arrived[SUM_B, si, j] = send(r.bsend.at[slot], r.brecv.at[slot], SUM_B, slot, peer)

    def third(si):
        value = r.keep[si]
        for j in range(1, sides):
            arrived[SUM_B, si, j].wait_recv()
            value = value + r.brecv[si * sides + j].astype(F32)
        if si == 0:
            return value
        r.zsend[si] = value.astype(BF16)
        arrived[SUM_Z, si] = send(
            r.zsend.at[si],
            r.zrecv.at[si],
            SUM_Z,
            si,
            device(lax.rem(z + si, zs), x, y, c),
        )
        return None

    for k, si in enumerate(zorder):
        second(si)
        if k:
            third(zorder[k - 1])
    final = third(0) + r.resid[...]
    for s in range(1, zs):
        arrived[SUM_Z, s].wait_recv()
        final = final + r.zrecv[s].astype(F32)
    r.out[...] = final.astype(BF16)
    for copy in waiting:
        copy.wait_send()
    for g in range(groups):
        pltpu.make_async_copy(
            r.st.at[span(g, ROWS)], r.new_state.at[span(g, ROWS)], r.stout.at[g]
        ).wait()


def place_kernel(held, held_state, out, new_state, buf, st, sems):
    size = held_state.shape[0]
    parts = [pl.ds(g * ROWS, ROWS) for g in range(size // ROWS)]
    moves = [(held, buf, out)]
    moves += [(held_state.at[p], st.at[p], new_state.at[p]) for p in parts]
    first = [
        pltpu.make_async_copy(src, mid, sems.at[0, k]) for k, (src, mid, _) in enumerate(moves)
    ]
    last = [
        pltpu.make_async_copy(mid, dst, sems.at[1, k]) for k, (_, mid, dst) in enumerate(moves)
    ]
    for copy in first:
        copy.start()
    for copy, after in zip(first, last):
        copy.wait()
        after.start()
    for copy in last:
        copy.wait()


def local(
    tokens,
    state,
    norm_gain,
    w_query,
    w_forget,
    w_input,
    w_outgate,
    lower_bound,
    head_gain,
    w_output,
    ffn_gain,
    route_ids,
    route_weight,
    expert_gate,
    expert_up,
    expert_down,
    shared_gate,
    shared_up,
    shared_down,
    dense_gate,
    dense_up,
    dense_down,
    dense_mix,
):
    n = lax.axis_size("ep")
    tpn = lax.axis_size("tp")
    sides = tpn // CORES
    zs = n // sides
    seq, width = tokens.shape
    depth, mixw = w_query.shape
    heads, hd = state.shape[1:3]
    cols = width // tpn
    half = sides * cols
    exp_local, _, ff = expert_gate.shape
    sff = shared_gate.shape[1]
    dff = dense_gate.shape[1] // tpn
    lanes = ceil_to(seq, LANES)
    rrows = ceil_to(exp_local, ROWS)
    groups = seq // ROWS
    move = dff % LANES == 0
    sds = jax.ShapeDtypeStruct
    VM, ANY = pltpu.VMEM, pl.ANY

    ins = dict(
        tokens=tokens,
        state=state,
        gain1=norm_gain[None, :],
        wq=w_query,
        wf=w_forget,
        wi=w_input,
        wo=w_outgate,
        lb=lower_bound[None, :],
        hg=head_gain[None, :],
        wout=w_output,
        gain2=ffn_gain[None, :],
        ids=route_ids.T,
        weights=route_weight.T,
        eg=expert_gate,
        eu=expert_up,
        ed=expert_down,
        sg=shared_gate,
        su=shared_up,
        sd=shared_down,
        mix=dense_mix[None, :],
    )
    if move:
        ins.update(dgate=dense_gate, dup=dense_up, ddown=dense_down)
    else:
        gate_w, up_w = [
            lax.all_to_all(w, "tp", split_axis=1, concat_axis=0, tiled=True)
            for w in (dense_gate, dense_up)
        ]
        down_w = lax.all_to_all(dense_down, "tp", split_axis=0, concat_axis=1, tiled=True)
        ins.update(gatew=gate_w, upw=up_w, downw=down_w)
    outs = dict(out=sds((seq, cols), BF16), new_state=sds(state.shape, F32))
    hops = zs * sides * sides
    scratch = dict(
        tokens_v=VM((seq, width), BF16),
        gain1_v=VM((1, width), F32),
        gain2_v=VM((1, width), F32),
        lb_v=VM((1, mixw), F32),
        hg_v=VM((1, mixw), F32),
        mix_v=VM((1, cols), F32),
        ids_v=VM(route_ids.shape[::-1], jnp.int32),
        weights_v=VM(route_weight.shape[::-1], F32),
        wout_v=VM((mixw, width), BF16),
        st=VM(state.shape, F32),
        nsend=VM((zs * seq, sides * depth), BF16),
        ncol=VM((zs * seq, sides * depth), BF16),
        wbuf=VM((4, sides * depth, mixw), BF16),
        psend=VM((4, zs * seq, mixw), BF16),
        precv=VM((4, zs * seq, mixw), BF16),
        dturn=VM((groups, mixw, ROWS), F32),
        qturn=VM((groups, mixw, ROWS), F32),
        vals=VM((seq, mixw), F32),
        read=VM((seq, mixw), F32),
        rsend=VM((n, rrows, lanes), F32),
        rrecv=VM((n, rrows, lanes), F32),
        mixs=VM((ROWS, cols), F32),
        mixr=VM((tpn, ROWS, cols), F32),
        hsend=VM((tpn, seq, cols), BF16),
        hrecv=VM((tpn, seq, cols), BF16),
        resid=VM((seq, cols), F32),
        rows=VM((CORES, n * seq, half), BF16),
        sqs=VM((ROWS, lanes), F32),
        sqr=VM((tpn, ROWS, lanes), F32),
        scs=VM((ROWS, lanes), F32),
        scr=VM((n, ROWS, lanes), F32),
        egv=VM((CORES, exp_local, half, ff), BF16),
        euv=VM((CORES, exp_local, half, ff), BF16),
        edv=VM((exp_local * ff, width), BF16),
        sgv=VM((CORES, half, sff), BF16),
        suv=VM((CORES, half, sff), BF16),
        sdv=VM((sff, width), BF16),
        dgv=VM((CORES, half, dff), BF16),
        duv=VM((CORES, half, dff), BF16),
        ddv=VM((tpn, dff, cols), BF16),
        acc=VM((2 * exp_local, n * seq, ff), F32),
        dacc=VM((2, n * seq, dff), F32),
        hid=VM((n * seq, exp_local * ff), BF16),
        dhid=VM((n * seq, dff), BF16),
        shared=VM((tpn, seq, cols), F32),
        part=VM((sides, n * seq, cols), BF16),
        crecv=VM((sides, n * seq, cols), BF16),
        both=VM((sides, n * seq, cols), BF16),
        arecv=VM((hops, seq, cols), BF16),
        keep=VM((zs, seq, cols), F32),
        bsend=VM((zs * sides, seq, cols), BF16),
        brecv=VM((zs * sides, seq, cols), BF16),
        zsend=VM((zs, seq, cols), BF16),
        zrecv=VM((zs, seq, cols), BF16),
        local=pltpu.SemaphoreType.DMA((64 + groups + 8 * exp_local * tpn,)),
        stout=pltpu.SemaphoreType.DMA((groups,)),
    )
    counts = {
        WEIGHT: 4 * sides,
        NORMED: zs,
        MOVE: 3 * tpn,
        ROUTE: n,
        MIX: tpn,
        PROJ: 4 * zs,
        HEAD: tpn,
        GATHER_Z: zs,
        GATHER_A: zs * sides,
        GATHER_B: hops,
        GATHER_C: hops,
        SQUARE: tpn,
        SCALE: n,
        SUM_C: sides,
        SUM_A: hops,
        SUM_B: zs * sides,
        SUM_Z: zs,
    }
    names = [*ins, *outs, *scratch]
    sems = [pltpu.SemaphoreType.DMA((counts[k],)) for k in range(len(counts)) for _ in range(2)]
    held = pl.pallas_call(
        functools.partial(layer_kernel, n, tpn, move, names),
        out_shape=tuple(outs.values()),
        in_specs=[pl.BlockSpec(memory_space=ANY) for _ in ins],
        out_specs=(pl.BlockSpec(memory_space=VM), pl.BlockSpec(memory_space=ANY)),
        scratch_shapes=list(scratch.values()) + sems,
        compiler_params=pltpu.CompilerParams(
            collective_id=0, has_side_effects=True, vmem_limit_bytes=VMEM_BYTES
        ),
    )(*ins.values())
    return pl.pallas_call(
        place_kernel,
        out_shape=tuple(outs.values()),
        in_specs=[pl.BlockSpec(memory_space=ANY)] * 2,
        out_specs=(pl.BlockSpec(memory_space=ANY),) * 2,
        scratch_shapes=[
            VM((seq, cols), BF16),
            VM(state.shape, F32),
            pltpu.SemaphoreType.DMA((2, groups + 1)),
        ],
        compiler_params=pltpu.CompilerParams(vmem_limit_bytes=VMEM_BYTES),
    )(*held)


def solution(mesh):
    placed = (
        P("ep", None),
        P("ep", "tp", None, None),
        P(),
        P("ep", "tp"),
        P("ep", "tp"),
        P("ep", "tp"),
        P("ep", "tp"),
        P("tp"),
        P("tp"),
        P("tp", None),
        P(),
        P("ep", None),
        P("ep", None),
        P("ep", None, "tp"),
        P("ep", None, "tp"),
        P("ep", "tp", None),
        P(None, "tp"),
        P(None, "tp"),
        P("tp", None),
        P("tp", "ep"),
        P("tp", "ep"),
        P("ep", "tp"),
        P("tp"),
    )
    return jax.shard_map(
        local,
        mesh=mesh,
        in_specs=placed,
        out_specs=(P("ep", "tp"), P("ep", "tp", None, None)),
        check_vma=False,
    )
```

```python
import functools
import types

import jax
import jax.numpy as jnp
from jax import lax
from jax.experimental import pallas as pl
from jax.experimental.pallas import tpu as pltpu
from jax.sharding import PartitionSpec as P

EPS = 1e-06
LANES = 128
CORES = 2
ROWS = 8
F32 = jnp.float32
BF16 = jnp.bfloat16
PIECES = 4
AHEAD = (13, 2)
PLACE_BYTES = 1024 * 1024
VMEM_BYTES = 52 * 1024 * 1024
(
    WEIGHT,
    NORMED,
    MOVE,
    ROUTE,
    HIDDEN_Y,
    HIDDEN_C,
    PROJ,
    HEAD,
    GATHER_Z,
    GATHER_A,
    GATHER_B,
    GATHER_C,
    SQUARE,
    SCALE,
    SUM_C,
    SUM_Y,
    SUM_X,
    SUM_Z,
) = range(18)


def span(index, size):
    if isinstance(index, int):
        return pl.ds(index * size, size)
    return pl.ds(pl.multiple_of(index * size, size), size)


def ceil_to(value, step):
    return -(-value // step) * step


def silu(v):
    return v * jax.nn.sigmoid(v)


def schedule(zs):
    Z, FIRST, SECOND, HALF, DENSE, EXPERT, DOWN, TWIN, HIDDEN, SUMS_Y, SUMS_X, SCALES, STATE = range(13)
    cost = (0.05, 0.05, 0.08, 0.5, 0.4, 0.6, 0.4, 0.53, 0.05, 0.37, 0.05, 0.1, 2.6)
    relays = (Z, FIRST, SECOND, SCALES, HIDDEN)
    after = {(STATE, 0): [], (SCALES, 0): [(None, 2.8)]}
    for k in range(zs):
        after[Z, k] = [(None, 2.8 + 1.6 * k if k else 0.0)]
        after[FIRST, k] = [((Z, k), 2.5)]
        after[SECOND, k] = [((FIRST, k), 2.5)]
        after[HALF, k] = [((SECOND, k), 0.0)]
        after[DENSE, k] = [((SECOND, k), 1.4), ((HALF, k), 0.0), ((SCALES, 0), 2.5)]
        after[EXPERT, k] = [((DENSE, k), 0.0)]
        after[DOWN, k] = [((EXPERT, k), 0.0)]
        after[TWIN, k] = [((DOWN, k), 1.4)]
        after[HIDDEN, k] = [((DENSE, k), 2.6)]
        after[SUMS_Y, k] = [((TWIN, k), 3.7), ((HIDDEN, k), 1.3)]
        after[SUMS_X, k] = [((SUMS_Y, k), 2.7)]
    done, now, order = {(Z, 0): 0.0, None: 0.0}, 0.0, []
    del after[Z, 0]
    while after:
        ready = {
            step: max([done[need] + wait for need, wait in needs] or [0.0])
            for step, needs in after.items()
            if all(need in done for need, _ in needs)
        }
        now = max(now, min(ready.values()))
        step = min(
            (step for step, at in ready.items() if at <= now),
            key=lambda step: (step[0] not in relays, step[0] == STATE, -step[0], step[1]),
        )
        now += cost[step[0]] + (0.8 if step == (DOWN, 0) else 0.0)
        done[step] = now
        order.append(step)
        del after[step]
    return order


def layer_kernel(n, tpn, move, names, *refs):
    sems = refs[len(names) :]
    r = types.SimpleNamespace(**dict(zip(names, refs)))
    me, tp = lax.axis_index("ep"), lax.axis_index("tp")
    sides = tpn // CORES
    xs = sides
    zs = n // xs
    z, x = lax.div(me, xs), lax.rem(me, xs)
    y, c = lax.div(tp, CORES), lax.rem(tp, CORES)
    twin_core = CORES - 1 - c
    seq, width = r.tokens.shape
    cols = width // tpn
    depth, mixw = r.wq.shape
    exp_local, _, ff = r.eg.shape
    sff = r.sg.shape[1]
    dff = r.dgv.shape[2]
    heads, hd = r.state.shape[1:3]
    wrap = xs * depth
    lanes = r.sqs.shape[1]
    half = sides * cols

    def pick(first, second):
        return first * (1 - c) + second * c

    def device(zz, xx, yy, cc):
        return {"ep": zz * xs + xx, "tp": yy * CORES + cc}

    waiting = []

    def send(src, dst, kind, slot, peer, landing=None):
        copy = pltpu.make_async_remote_copy(
            src_ref=src,
            dst_ref=dst,
            send_sem=sems[2 * kind].at[slot],
            recv_sem=sems[2 * kind + 1].at[slot if landing is None else landing],
            device_id=peer,
            device_id_type=pl.DeviceIdType.MESH,
        )
        copy.start()
        waiting.append(copy)
        return copy

    def landed(kind, slot, ref):
        pltpu.make_async_remote_copy(
            src_ref=ref,
            dst_ref=ref,
            send_sem=sems[2 * kind].at[slot],
            recv_sem=sems[2 * kind + 1].at[slot],
            device_id=device(z, x, y, twin_core),
            device_id_type=pl.DeviceIdType.MESH,
        ).wait_recv()

    high = lax.div(2 * z, zs)
    near = z * (1 - high) + (zs - 1 - z) * high

    def zat(k):
        if k == 0:
            return z
        place = k - 1 + lax.div(zs + k - 1 - near, zs)
        return place * (1 - high) + (zs - 1 - place) * high

    far_first = range(zs - 1, 0, -1)
    used = [0]

    def fetch(src, dst):
        copy = pltpu.make_async_copy(src, dst, r.local.at[used[0]])
        used[0] += 1
        copy.start()
        return copy

    got = types.SimpleNamespace()
    got.tokens = fetch(r.tokens, r.tokens_v)
    got.gain1 = fetch(r.gain1, r.gain1_v)
    order = (r.wf, r.wq, r.wi, r.wo)
    got.w = [fetch(w, r.wbuf.at[i, span(x, depth), :]) for i, w in enumerate(order)]
    got.lb = fetch(r.lb, r.lb_v)
    got.hg = fetch(r.hg, r.hg_v)
    got.mix = fetch(r.mix, r.mix_v)
    got.ids = fetch(r.ids, r.ids_v)
    got.weights = fetch(r.weights, r.weights_v)
    groups = seq // ROWS
    states = [
        fetch(r.state.at[pl.ds(g * ROWS, ROWS)], r.new_state.at[pl.ds(g * ROWS, ROWS)])
        for g in range(groups)
    ]
    got.wout = fetch(r.wout, r.wout_v)
    got.gain2 = fetch(r.gain2, r.gain2_v)

    barrier = pltpu.get_barrier_semaphore()
    for s in range(1, tpn):
        pl.semaphore_signal(
            barrier,
            inc=1,
            device_id={"tp": lax.rem(tp + s, tpn)},
            device_id_type=pl.DeviceIdType.MESH,
        )
    for s in range(1, n):
        pl.semaphore_signal(
            barrier,
            inc=1,
            device_id={"ep": lax.rem(me + s, n)},
            device_id_type=pl.DeviceIdType.MESH,
        )
    got.tokens.wait()
    got.gain1.wait()
    t32 = r.tokens_v[...].astype(F32)
    normed = (
        t32 * lax.rsqrt(jnp.mean(t32 * t32, axis=-1, keepdims=True) + EPS) * r.gain1_v[...]
    ).astype(BF16)
    for d in range(zs):
        r.nsend[d * seq : (d + 1) * seq, :] = normed[:, d * wrap : (d + 1) * wrap]
    r.ncol[span(z, seq), :] = r.nsend[span(z, seq), :]
    pl.semaphore_wait(barrier, n - 1 + tpn - 1)

    arrived = {}
    for i, w in enumerate(order):
        for s in range(1, xs):
            arrived[WEIGHT, i, s] = send(
                w,
                r.wbuf.at[i, span(x, depth), :],
                WEIGHT,
                i * xs + s,
                device(z, lax.rem(x + s, xs), y, c),
            )
    for k in far_first:
        zz = zat(k)
        send(
            r.nsend.at[span(zz, seq)],
            r.ncol.at[span(z, seq)],
            NORMED,
            k,
            device(zz, x, y, c),
            z,
        )
    pieces = []
    if move:
        rows = r.dgate.shape[0]
        got.dgv = []
        for i, (src, dst) in enumerate(((r.dgate, r.dgv), (r.dup, r.duv))):
            for q in range(sides):
                for k in range(CORES):
                    core = twin_core if k else c
                    peer = lax.rem(y + q, sides) * CORES + core
                    count = PIECES if q else 1
                    size = rows // count
                    for j in range(count):
                        part = pl.ds(j * size, size)
                        a = src.at[part, span(peer, dff)]
                        b = dst.at[c, pl.ds(pl.multiple_of(y * rows + j * size, ROWS), size), :]
                        slot = ((i * sides + q) * CORES + k) * PIECES + j
                        if q:
                            pieces.append((a, b, slot, peer, i))
                        elif k:
                            arrived[MOVE, i, slot] = send(a, b, MOVE, slot, {"tp": peer})
                        else:
                            got.dgv.append(fetch(a, b))

    def move_pieces(count):
        for a, b, slot, peer, i in pieces[:count]:
            arrived[MOVE, i, slot] = send(a, b, MOVE, slot, {"tp": peer})
        del pieces[:count]

    def moved():
        for key, copy in arrived.items():
            if key[0] == MOVE:
                copy.wait_recv()

    move_pieces(AHEAD[0])

    got.ids.wait()
    got.weights.wait()
    got.mix.wait()
    eye = lax.broadcasted_iota(jnp.int32, (seq, lanes), 0) == lax.broadcasted_iota(
        jnp.int32, (seq, lanes), 1
    )
    ids, weights = r.ids_v[...], r.weights_v[...]
    rrows = r.rsend.shape[1]

    def to_row(col):
        return jnp.sum(jnp.where(eye, col, 0.0), axis=0, keepdims=True)

    def to_col(row):
        return jnp.sum(jnp.where(eye, row, 0.0), axis=1, keepdims=True)

    for d in range(n):
        r.rsend[d] = jnp.zeros((rrows, lanes), F32)
        for i in range(exp_local):
            r.rsend[d, i : i + 1, :seq] = jnp.sum(
                jnp.where(ids == d * exp_local + i, weights, 0.0), axis=0, keepdims=True
            )
    r.rrecv[me] = r.rsend[me]
    for s in range(1, n):
        peer = lax.rem(me + s, n)
        arrived[ROUTE, s] = send(
            r.rsend.at[peer], r.rrecv.at[me], ROUTE, s, {"ep": peer}
        )
    def fetch_rows(src, dst):
        return [
            fetch(src.at[span(t, cols), :], dst(t % CORES).at[span(t // CORES, cols), :])
            for t in range(tpn)
        ]

    got.sgv = fetch_rows(r.sg, lambda k: r.sgv.at[k]) + fetch_rows(r.su, lambda k: r.suv.at[k])
    got.sdv = [fetch(r.sd, r.sdv)]
    got.egv = []
    for e in range(exp_local):
        got.egv += fetch_rows(r.eg.at[e], lambda k: r.egv.at[k, e])
        got.egv += fetch_rows(r.eu.at[e], lambda k: r.euv.at[k, e])
    got.edv = [fetch(r.ed.at[e], r.edv.at[span(e, ff), :]) for e in range(exp_local)]
    got.ddv = fetch(r.ddown, r.ddv)
    if not move:
        got.dgv = fetch_rows(r.gatew, lambda k: r.dgv.at[k])
        got.dgv += fetch_rows(r.upw, lambda k: r.duv.at[k])

    for k in range(1, zs):
        landed(NORMED, zat(k), r.ncol.at[span(zat(k), seq)])
    for i in range(len(order)):
        got.w[i].wait()
        for s in range(1, xs):
            arrived[WEIGHT, i, s].wait_recv()
        r.psend[i] = jnp.dot(
            r.ncol[...], r.wbuf[i], preferred_element_type=F32
        ).astype(BF16)
        for k in far_first:
            zz = zat(k)
            send(
                r.psend.at[i, span(zz, seq)],
                r.precv.at[i, span(z, seq)],
                PROJ,
                i * zs + k,
                device(zz, x, y, c),
                i * zs + z,
            )

    def projected(i):
        total = r.psend[i, span(z, seq), :].astype(F32)
        for k in range(1, zs):
            zz = zat(k)
            landed(PROJ, i * zs + zz, r.precv.at[i, span(zz, seq)])
            total = total + r.precv[i, span(zz, seq), :].astype(F32)
        return total.astype(BF16).astype(F32)

    padded = ceil_to(seq, LANES)

    def turn(value, dst):
        if padded > seq:
            value = jnp.concatenate([value, jnp.zeros((padded - seq, mixw), F32)], axis=0)
        value = value.T
        for g in range(groups):
            dst[g] = value[:, g * ROWS : (g + 1) * ROWS]

    got.lb.wait()
    got.hg.wait()
    lb = r.lb_v[...]
    decay = lb + (1.0 - lb) * jax.nn.sigmoid(projected(0))
    query = projected(1)
    turn(decay, r.dturn)
    turn(query * decay, r.qturn)
    keyed = query * (1.0 - decay)
    for copy in states:
        copy.wait()

    def read_group(g, carry):
        qg = r.qturn[g]
        rows = []
        for b in range(ROWS):
            parts = [
                jnp.sum(
                    qg[h * hd : (h + 1) * hd, b : b + 1] * r.new_state[g * ROWS + b, h],
                    axis=0,
                    keepdims=True,
                )
                for h in range(heads)
            ]
            rows.append(jnp.concatenate(parts, axis=1))
        r.read[span(g, ROWS), :] = jnp.concatenate(rows, axis=0)
        return carry

    lax.fori_loop(0, groups, read_group, 0)

    def write_group(g, carry):
        dg = r.dturn[g]
        vg = r.vals[span(g, ROWS), :]
        for b in range(ROWS):
            for h in range(heads):
                at = slice(h * hd, (h + 1) * hd)
                vrow = vg[b : b + 1, at]
                old = r.new_state[g * ROWS + b, h]
                r.new_state[g * ROWS + b, h] = vrow + dg[at, b : b + 1] * (old - vrow)
        return carry

    values = projected(2)
    r.vals[...] = values
    read = r.read[...]
    parts = []
    for h in range(heads):
        at = slice(h * hd, (h + 1) * hd)
        part = read[:, at] + jnp.sum(keyed[:, at], axis=-1, keepdims=True) * values[:, at]
        parts.append(part * lax.rsqrt(jnp.mean(part * part, axis=-1, keepdims=True) + EPS))
    read = jnp.concatenate(parts, axis=1)
    head = (read * r.hg_v[...] * silu(projected(3))).astype(BF16)

    got.wout.wait()
    got.gain2.wait()
    for t in range(tpn):
        r.hsend[t] = jnp.dot(
            head, r.wout_v[:, t * cols : (t + 1) * cols], preferred_element_type=F32
        ).astype(BF16)
    for s in range(1, tpn):
        peer = lax.rem(tp + s, tpn)
        arrived[HEAD, s] = send(r.hsend.at[peer], r.hrecv.at[tp], HEAD, s, {"tp": peer})
    move_pieces(AHEAD[1])
    mine = span(tp, cols)
    total = r.tokens_v[:, mine].astype(F32) + r.hsend[tp].astype(F32)
    for s in range(1, tpn):
        arrived[HEAD, s].wait_recv()
        total = total + r.hrecv[lax.rem(tp + tpn - s, tpn)].astype(F32)
    r.resid[...] = total

    def block(zz, xx, yy, cc):
        return r.rows.at[cc, span(zz * xs + xx, seq), span(yy, cols)]

    r.rows[c, span(me, seq), span(y, cols)] = (total * r.gain2_v[:, mine]).astype(BF16)
    own = block(z, x, y, c)
    for k in far_first:
        send(own, own, GATHER_Z, k, device(zat(k), x, y, c), z)

    def plane(k, a, b):
        xx = lax.rem(x + xs - pick(a, b), xs)
        yy = lax.rem(y + sides - pick(b, a), sides)
        return block(zat(k), xx, yy, c)

    def forward_first(k):
        ref = plane(k, 0, 0)
        for q in range(1, sides):
            peer = device(z, lax.rem(x + pick(q, 0), xs), lax.rem(y + pick(0, q), sides), c)
            arrived[GATHER_A, k, q] = send(ref, ref, GATHER_A, k * sides + q, peer)

    def forward_second(k, a):
        ref = plane(k, a, 0)
        for q in range(1, sides):
            peer = device(z, lax.rem(x + pick(0, q), xs), lax.rem(y + pick(q, 0), sides), c)
            arrived[GATHER_B, k, a, q] = send(
                ref, ref, GATHER_B, (k * sides + a) * sides + q, peer
            )

    def forward_twin(k, a, b):
        ref = plane(k, a, b)
        arrived[GATHER_C, k, a, b] = send(
            ref, ref, GATHER_C, (k * sides + a) * sides + b, device(z, x, y, twin_core)
        )

    forward_first(0)
    forward_second(0, 0)
    forward_twin(0, 0, 0)
    move_pieces(len(pieces))

    square = to_row(jnp.sum(total * total, axis=-1, keepdims=True))
    r.sqs[...] = jnp.broadcast_to(square, (ROWS, lanes))
    for s in range(1, tpn):
        arrived[SQUARE, s] = send(
            r.sqs, r.sqr.at[tp], SQUARE, s, {"tp": lax.rem(tp + s, tpn)}
        )
    size = xs * seq
    pairs = [(r.egv, r.euv, e) for e in range(exp_local)] + [(r.dgv, r.duv, None)]

    def weight(ref, lead, core):
        return ref[core] if lead is None else ref[core, lead]

    def scale_out(k):
        square = r.sqs[:1]
        for s in range(1, tpn):
            arrived[SQUARE, s].wait_recv()
            square = square + r.sqr[lax.rem(tp + tpn - s, tpn)][:1]
        r.scr[me] = jnp.broadcast_to(lax.rsqrt(square / width + EPS), (ROWS, lanes))
        for s in range(1, n):
            send(r.scr.at[me], r.scr.at[me], SCALE, s, {"ep": lax.rem(me + s, n)}, me)

    def from_z(k):
        landed(GATHER_Z, zat(k), plane(k, 0, 0))
        forward_first(k)
        forward_second(k, 0)
        forward_twin(k, 0, 0)

    def from_first(k):
        for a in range(1, sides):
            arrived[GATHER_A, k, a].wait_recv()
            forward_second(k, a)
            forward_twin(k, a, 0)

    def from_second(k):
        for a in range(sides):
            for b in range(1, sides):
                arrived[GATHER_B, k, a, b].wait_recv()
                forward_twin(k, a, b)

    def first_half(k):
        if k == 0:
            for copy in got.egv + got.dgv:
                copy.wait()
            moved()
        lhs = r.rows[c, span(zat(k), size), :]
        for i, (gate, up, lead) in enumerate(pairs):
            for j, ref in enumerate((gate, up)):
                product = jnp.dot(lhs, weight(ref, lead, c), preferred_element_type=F32)
                if lead is None:
                    r.dacc[j, k] = product
                else:
                    r.acc[2 * i + j, k] = product

    def column(ref, k, row):
        return jnp.concatenate(
            [to_col(ref[zat(k) * xs + i][row : row + 1]) for i in range(xs)], axis=0
        )

    def shared_expert():
        for copy in got.sgv + got.sdv:
            copy.wait()
        pre = [
            sum(
                jnp.dot(r.rows[k, span(me, seq), :], ref[k], preferred_element_type=F32)
                for k in range(CORES)
            )
            for ref in (r.sgv, r.suv)
        ]
        own_scale = to_col(r.scr[me][:1])
        hidden = (silu(own_scale * pre[0]) * (own_scale * pre[1])).astype(BF16)
        for t in range(tpn):
            r.shared[t] = jnp.dot(
                hidden, r.sdv[:, t * cols : (t + 1) * cols], preferred_element_type=F32
            )

    def partial(k, yy, cc):
        t = yy * CORES + cc
        value = jnp.dot(r.hid[k], r.edv[:, span(t, cols)], preferred_element_type=F32)
        if k == 0:
            r.wide[...] = value
            r.wide[span(x, seq), :] = r.wide[span(x, seq), :] + r.shared[t]
            value = r.wide[...]
        return value

    def dense_half(k):
        for a in range(sides):
            for b in range(sides):
                arrived[GATHER_C, k, a, b].wait_recv()
        if k == 0:
            for s in range(1, n):
                arrived[ROUTE, s].wait_recv()
        for i in range(xs):
            if k or i:
                e = zat(k) * xs + lax.rem(x + i, xs)
                landed(SCALE, e, r.scr.at[e])
        hidden_of(k, len(pairs) - 1)

    def expert_half(k):
        for i in range(exp_local):
            hidden_of(k, i)

    def hidden_of(k, i):
        scale = column(r.scr, k, 0)
        lhs = r.rows[twin_core, span(zat(k), size), :]
        gate, up, lead = pairs[i]
        both = []
        for j, ref in enumerate((gate, up)):
            before = r.dacc[j, k] if lead is None else r.acc[2 * i + j, k]
            product = jnp.dot(lhs, weight(ref, lead, twin_core), preferred_element_type=F32)
            both.append(scale * (before + product))
        hidden = silu(both[0]) * both[1]
        if lead is None:
            r.dhid[k, tp] = hidden.astype(BF16)
            ref = r.dhid.at[k, tp]
            for q in range(1, sides):
                peer = device(z, x, lax.rem(y + q, sides), c)
                arrived[HIDDEN_Y, k, q] = send(ref, ref, HIDDEN_Y, k * sides + q, peer)
            arrived[HIDDEN_C, k, 0] = send(
                ref, ref, HIDDEN_C, k * sides, device(z, x, y, twin_core)
            )
        else:
            share = column(r.rrecv, k, lead)
            r.hid[k, :, i * ff : (i + 1) * ff] = (hidden * share).astype(BF16)

    def down(k):
        if k == 0:
            for copy in got.edv:
                copy.wait()
            shared_expert()
        for q in [*range(1, sides), 0]:
            slot = k * sides + q
            r.part[slot] = partial(k, lax.rem(y + q, sides), twin_core).astype(BF16)
            arrived[SUM_C, k, q] = send(
                r.part.at[slot], r.crecv.at[slot], SUM_C, slot, device(z, x, y, twin_core)
            )

    def hidden_on(k):
        for q in range(1, sides):
            arrived[HIDDEN_Y, k, q].wait_recv()
            ref = r.dhid.at[k, lax.rem(y + sides - q, sides) * CORES + c]
            arrived[HIDDEN_C, k, q] = send(
                ref, ref, HIDDEN_C, k * sides + q, device(z, x, y, twin_core)
            )

    def from_twin(k):
        for q in [*range(1, sides), 0]:
            slot = k * sides + q
            yy = lax.rem(y + q, sides)
            value = partial(k, yy, c)
            arrived[SUM_C, k, q].wait_recv()
            value = value + r.crecv[slot].astype(F32)
            if q == 0:
                r.keep[k] = value
                continue
            r.ysend[slot] = value.astype(BF16)
            arrived[SUM_Y, k, q] = send(
                r.ysend.at[slot], r.yrecv.at[slot], SUM_Y, slot, device(z, x, yy, c)
            )

    def from_y(k):
        for q in range(sides):
            arrived[HIDDEN_C, k, q].wait_recv()
        if k == 0:
            got.ddv.wait()
        dense = sum(
            jnp.dot(
                r.dhid[k, t], r.ddv[t * dff : (t + 1) * dff, :], preferred_element_type=F32
            )
            for t in range(tpn)
        )
        value = r.keep[k] + jax.nn.sigmoid(r.mix_v[...]) * dense
        for q in range(1, sides):
            arrived[SUM_Y, k, q].wait_recv()
            value = value + r.yrecv[k * sides + q].astype(F32)
        r.keep[k] = value
        for q in range(1, xs):
            slot = k * sides + q
            xx = lax.rem(x + q, xs)
            r.xsend[slot] = r.keep[k, span(xx, seq), :].astype(BF16)
            arrived[SUM_X, k, q] = send(
                r.xsend.at[slot], r.xrecv.at[slot], SUM_X, slot, device(z, xx, y, c)
            )

    def from_x(k):
        value = r.keep[k, span(x, seq), :]
        for q in range(1, xs):
            arrived[SUM_X, k, q].wait_recv()
            value = value + r.xrecv[k * sides + q].astype(F32)
        if k == 0:
            r.resid[...] = r.resid[...] + value
        else:
            r.zsend[k] = value.astype(BF16)
            send(r.zsend.at[k], r.zrecv.at[z], SUM_Z, k, device(zat(k), x, y, c), z)

    def write_state(k):
        lax.fori_loop(0, groups, write_group, 0)

    kinds = (
        from_z, from_first, from_second, first_half, dense_half, expert_half, down,
        from_twin, hidden_on, from_y, from_x, scale_out, write_state,
    )
    for kind, k in schedule(zs):
        step = kinds[kind]
        step(k)

    final = r.resid[...]
    for k in range(1, zs):
        landed(SUM_Z, zat(k), r.zrecv.at[zat(k)])
        final = final + r.zrecv[zat(k)].astype(F32)
    r.out[...] = final.astype(BF16)

    for copy in waiting:
        copy.wait_send()


def place_kernel(held, held_state, out, new_state, sems):
    parts = [pl.ds(g * ROWS, ROWS) for g in range(held_state.shape[0] // ROWS)]
    moves = [(held_state.at[p], new_state.at[p]) for p in parts] + [(held, out)]
    copies = [pltpu.make_async_copy(*move, sems.at[k]) for k, move in enumerate(moves)]
    for copy in copies:
        copy.start()
    for copy in copies:
        copy.wait()


def local(
    tokens,
    state,
    norm_gain,
    w_query,
    w_forget,
    w_input,
    w_outgate,
    lower_bound,
    head_gain,
    w_output,
    ffn_gain,
    route_ids,
    route_weight,
    expert_gate,
    expert_up,
    expert_down,
    shared_gate,
    shared_up,
    shared_down,
    dense_gate,
    dense_up,
    dense_down,
    dense_mix,
):
    n = lax.axis_size("ep")
    tpn = lax.axis_size("tp")
    sides = tpn // CORES
    zs = n // sides
    seq, width = tokens.shape
    depth, mixw = w_query.shape
    heads, hd = state.shape[1:3]
    cols = width // tpn
    half = sides * cols
    exp_local, _, ff = expert_gate.shape
    sff = shared_gate.shape[1]
    dff = dense_gate.shape[1] // tpn
    lanes = ceil_to(seq, LANES)
    rrows = ceil_to(exp_local, ROWS)
    groups = seq // ROWS
    move = dff % LANES == 0
    sds = jax.ShapeDtypeStruct
    VM, ANY = pltpu.VMEM, pl.ANY

    ins = dict(
        tokens=tokens,
        state=state,
        gain1=norm_gain[None, :],
        wq=w_query,
        wf=w_forget,
        wi=w_input,
        wo=w_outgate,
        lb=lower_bound[None, :],
        hg=head_gain[None, :],
        wout=w_output,
        gain2=ffn_gain[None, :],
        ids=route_ids.T,
        weights=route_weight.T,
        eg=expert_gate,
        eu=expert_up,
        ed=expert_down,
        sg=shared_gate,
        su=shared_up,
        sd=shared_down,
        mix=dense_mix[None, :],
        ddown=dense_down,
    )
    if move:
        ins.update(dgate=dense_gate, dup=dense_up)
    else:
        gate_w, up_w = [
            lax.all_to_all(w, "tp", split_axis=1, concat_axis=0, tiled=True)
            for w in (dense_gate, dense_up)
        ]
        ins.update(gatew=gate_w, upw=up_w)
    outs = dict(out=sds((seq, cols), BF16), new_state=sds(state.shape, F32))
    hops = zs * sides * sides
    size = sides * seq
    scratch = dict(
        tokens_v=VM((seq, width), BF16),
        gain1_v=VM((1, width), F32),
        gain2_v=VM((1, width), F32),
        lb_v=VM((1, mixw), F32),
        hg_v=VM((1, mixw), F32),
        mix_v=VM((1, cols), F32),
        ids_v=VM(route_ids.shape[::-1], jnp.int32),
        weights_v=VM(route_weight.shape[::-1], F32),
        wout_v=VM((mixw, width), BF16),
        nsend=VM((zs * seq, sides * depth), BF16),
        ncol=VM((zs * seq, sides * depth), BF16),
        wbuf=VM((4, sides * depth, mixw), BF16),
        psend=VM((4, zs * seq, mixw), BF16),
        precv=VM((4, zs * seq, mixw), BF16),
        dturn=VM((groups, mixw, ROWS), F32),
        qturn=VM((groups, mixw, ROWS), F32),
        vals=VM((seq, mixw), F32),
        read=VM((seq, mixw), F32),
        rsend=VM((n, rrows, lanes), F32),
        rrecv=VM((n, rrows, lanes), F32),
        hsend=VM((tpn, seq, cols), BF16),
        hrecv=VM((tpn, seq, cols), BF16),
        resid=VM((seq, cols), F32),
        rows=VM((CORES, n * seq, half), BF16),
        sqs=VM((ROWS, lanes), F32),
        sqr=VM((tpn, ROWS, lanes), F32),
        scr=VM((n, ROWS, lanes), F32),
        egv=VM((CORES, exp_local, half, ff), BF16),
        euv=VM((CORES, exp_local, half, ff), BF16),
        edv=VM((exp_local * ff, width), BF16),
        sgv=VM((CORES, half, sff), BF16),
        suv=VM((CORES, half, sff), BF16),
        sdv=VM((sff, width), BF16),
        dgv=VM((CORES, half, dff), BF16),
        duv=VM((CORES, half, dff), BF16),
        ddv=VM(dense_down.shape, BF16),
        acc=VM((2 * exp_local, zs, size, ff), F32),
        dacc=VM((2, zs, size, dff), F32),
        hid=VM((zs, size, exp_local * ff), BF16),
        dhid=VM((zs, tpn, size, dff), BF16),
        wide=VM((size, cols), F32),
        part=VM((zs * sides, size, cols), BF16),
        crecv=VM((zs * sides, size, cols), BF16),
        ysend=VM((zs * sides, size, cols), BF16),
        yrecv=VM((zs * sides, size, cols), BF16),
        keep=VM((zs, size, cols), F32),
        xsend=VM((zs * sides, seq, cols), BF16),
        xrecv=VM((zs * sides, seq, cols), BF16),
        zsend=VM((zs, seq, cols), BF16),
        zrecv=VM((zs, seq, cols), BF16),
        shared=VM((tpn, seq, cols), F32),
        local=pltpu.SemaphoreType.DMA((64 + groups + 8 * exp_local * tpn,)),
    )
    counts = {
        WEIGHT: 4 * sides,
        NORMED: zs,
        MOVE: 2 * tpn * PIECES,
        ROUTE: n,
        HIDDEN_Y: zs * sides,
        HIDDEN_C: zs * sides,
        PROJ: 4 * zs,
        HEAD: tpn,
        GATHER_Z: zs,
        GATHER_A: zs * sides,
        GATHER_B: hops,
        GATHER_C: hops,
        SQUARE: tpn,
        SCALE: n,
        SUM_C: zs * sides,
        SUM_Y: zs * sides,
        SUM_X: zs * sides,
        SUM_Z: zs,
    }
    names = [*ins, *outs, *scratch]
    sems = [pltpu.SemaphoreType.DMA((counts[k],)) for k in range(len(counts)) for _ in range(2)]
    held = pl.pallas_call(
        functools.partial(layer_kernel, n, tpn, move, names),
        out_shape=tuple(VM(out.shape, out.dtype) for out in outs.values()),
        in_specs=[pl.BlockSpec(memory_space=ANY) for _ in ins],
        out_specs=(pl.BlockSpec(memory_space=VM),) * 2,
        scratch_shapes=list(scratch.values()) + sems,
        compiler_params=pltpu.CompilerParams(
            collective_id=0, has_side_effects=True, vmem_limit_bytes=VMEM_BYTES
        ),
    )(*ins.values())
    return pl.pallas_call(
        place_kernel,
        out_shape=tuple(outs.values()),
        in_specs=[pl.BlockSpec(memory_space=VM)] * 2,
        out_specs=(pl.BlockSpec(memory_space=ANY),) * 2,
        scratch_shapes=[pltpu.SemaphoreType.DMA((groups + 1,))],
        compiler_params=pltpu.CompilerParams(vmem_limit_bytes=PLACE_BYTES),
    )(*[pltpu.with_memory_space_constraint(a, VM) for a in held])


def solution(mesh):
    placed = (
        P("ep", None),
        P("ep", "tp", None, None),
        P(),
        P("ep", "tp"),
        P("ep", "tp"),
        P("ep", "tp"),
        P("ep", "tp"),
        P("tp"),
        P("tp"),
        P("tp", None),
        P(),
        P("ep", None),
        P("ep", None),
        P("ep", None, "tp"),
        P("ep", None, "tp"),
        P("ep", "tp", None),
        P(None, "tp"),
        P(None, "tp"),
        P("tp", None),
        P("tp", "ep"),
        P("tp", "ep"),
        P("ep", "tp"),
        P("tp"),
    )
    return jax.shard_map(
        local,
        mesh=mesh,
        in_specs=placed,
        out_specs=(P("ep", "tp"), P("ep", "tp", None, None)),
        check_vma=False,
    )
```

```python
import functools
import types

import jax
import jax.numpy as jnp
from jax import lax
from jax.experimental import pallas as pl
from jax.experimental.pallas import tpu as pltpu
from jax.sharding import PartitionSpec as P

EPS = 1e-06
LANES = 128
CORES = 2
ROWS = 8
F32 = jnp.float32
BF16 = jnp.bfloat16
PIECES = 4
AHEAD = (12, 2, 2)
MOVED_AT = 10.0
PLACE_BYTES = 1024 * 1024
VMEM_BYTES = 52 * 1024 * 1024
(
    WEIGHT,
    NORMED,
    MOVE,
    ROUTE,
    HIDDEN_Y,
    HIDDEN_C,
    PROJ,
    HEAD,
    GATHER_Z,
    GATHER_P,
    GATHER_C,
    SQUARE,
    SCALE,
    SUM_C,
    SUM_P,
    SUM_Z,
) = range(16)


def span(index, size):
    if isinstance(index, int):
        return pl.ds(index * size, size)
    return pl.ds(pl.multiple_of(index * size, size), size)


def ceil_to(value, step):
    return -(-value // step) * step


def silu(v):
    return v * jax.nn.sigmoid(v)


def schedule(zs):
    Z, PLANE, HALF, SECOND, DOWN, DENSE, TWIN, HIDDEN, ADD, SUMS, SCALES, STATE = range(12)
    cost = (0.05, 0.08, 0.4, 0.55, 0.35, 0.55, 0.5, 0.05, 0.35, 0.05, 0.1, 2.1)
    relays = (Z, PLANE, SCALES, HIDDEN)
    after = {(STATE, 0): [], (SCALES, 0): [(None, 2.5)]}
    for k in range(zs):
        after[Z, k] = [(None, 2.8 + 1.6 * k if k else 0.0)]
        after[PLANE, k] = [((Z, k), 3.2)]
        after[HALF, k] = [((PLANE, k), 0.0)]
        after[SECOND, k] = [((PLANE, k), 1.4), ((HALF, k), 0.0), ((SCALES, 0), 2.5)]
        after[DOWN, k] = [((SECOND, k), 0.0)]
        after[DENSE, k] = [((SECOND, k), 0.0), (None, MOVED_AT)]
        after[TWIN, k] = [((DOWN, k), 1.4)]
        after[HIDDEN, k] = [((DENSE, k), 4.0)]
        after[ADD, k] = [((TWIN, k), 0.0), ((HIDDEN, k), 1.3)]
        after[SUMS, k] = [((TWIN, k), 3.6), ((ADD, k), 2.9)]
    done, now, order = {(Z, 0): 0.0, None: 0.0}, 0.0, []
    del after[Z, 0]
    while after:
        ready = {
            step: max([done[need] + wait for need, wait in needs] or [0.0])
            for step, needs in after.items()
            if all(need in done for need, _ in needs)
        }
        now = max(now, min(ready.values()))
        step = min(
            (step for step, at in ready.items() if at <= now),
            key=lambda step: (step[0] not in relays, step[0] == STATE, step[0] in (ADD, TWIN), -step[0], step[1]),
        )
        now += cost[step[0]] + (0.8 if step == (DOWN, 0) else 0.0)
        done[step] = now
        order.append(step)
        del after[step]
    return order


def layer_kernel(n, tpn, move, names, *refs):
    sems = refs[len(names) :]
    r = types.SimpleNamespace(**dict(zip(names, refs)))
    me, tp = lax.axis_index("ep"), lax.axis_index("tp")
    sides = tpn // CORES
    xs = sides
    zs = n // xs
    z, x = lax.div(me, xs), lax.rem(me, xs)
    y, c = lax.div(tp, CORES), lax.rem(tp, CORES)
    twin_core = CORES - 1 - c
    seq, width = r.tokens.shape
    cols = width // tpn
    depth, mixw = r.wq.shape
    exp_local, _, ff = r.eg.shape
    sff = r.sg.shape[1]
    dff = r.dgv.shape[2]
    heads, hd = r.state.shape[1:3]
    wrap = xs * depth
    lanes = r.sqs.shape[1]
    half = sides * cols

    def device(zz, xx, yy, cc):
        return {"ep": zz * xs + xx, "tp": yy * CORES + cc}

    waiting = []

    def send(src, dst, kind, slot, peer, landing=None):
        copy = pltpu.make_async_remote_copy(
            src_ref=src,
            dst_ref=dst,
            send_sem=sems[2 * kind].at[slot],
            recv_sem=sems[2 * kind + 1].at[slot if landing is None else landing],
            device_id=peer,
            device_id_type=pl.DeviceIdType.MESH,
        )
        copy.start()
        waiting.append(copy)
        return copy

    def landed(kind, slot, ref):
        pltpu.make_async_remote_copy(
            src_ref=ref,
            dst_ref=ref,
            send_sem=sems[2 * kind].at[slot],
            recv_sem=sems[2 * kind + 1].at[slot],
            device_id=device(z, x, y, twin_core),
            device_id_type=pl.DeviceIdType.MESH,
        ).wait_recv()

    high = lax.div(2 * z, zs)
    near = z * (1 - high) + (zs - 1 - z) * high

    def zat(k):
        if k == 0:
            return z
        place = k - 1 + lax.div(zs + k - 1 - near, zs)
        return place * (1 - high) + (zs - 1 - place) * high

    far_first = range(zs - 1, 0, -1)
    used = [0]

    def fetch(src, dst):
        copy = pltpu.make_async_copy(src, dst, r.local.at[used[0]])
        used[0] += 1
        copy.start()
        return copy

    got = types.SimpleNamespace()
    got.tokens = fetch(r.tokens, r.tokens_v)
    got.gain1 = fetch(r.gain1, r.gain1_v)
    order = (r.wf, r.wq, r.wi, r.wo)
    got.w = [fetch(w, r.wbuf.at[i, span(x, depth), :]) for i, w in enumerate(order)]
    got.lb = fetch(r.lb, r.lb_v)
    got.hg = fetch(r.hg, r.hg_v)
    got.mix = fetch(r.mix, r.mix_v)
    got.ids = fetch(r.ids, r.ids_v)
    got.weights = fetch(r.weights, r.weights_v)
    groups = seq // ROWS
    states = [
        fetch(r.state.at[pl.ds(g * ROWS, ROWS)], r.new_state.at[pl.ds(g * ROWS, ROWS)])
        for g in range(groups)
    ]
    got.wout = fetch(r.wout, r.wout_v)
    got.gain2 = fetch(r.gain2, r.gain2_v)

    barrier = pltpu.get_barrier_semaphore()
    for s in range(1, tpn):
        pl.semaphore_signal(
            barrier,
            inc=1,
            device_id={"tp": lax.rem(tp + s, tpn)},
            device_id_type=pl.DeviceIdType.MESH,
        )
    for s in range(1, n):
        pl.semaphore_signal(
            barrier,
            inc=1,
            device_id={"ep": lax.rem(me + s, n)},
            device_id_type=pl.DeviceIdType.MESH,
        )
    got.tokens.wait()
    got.gain1.wait()
    t32 = r.tokens_v[...].astype(F32)
    normed = (
        t32 * lax.rsqrt(jnp.mean(t32 * t32, axis=-1, keepdims=True) + EPS) * r.gain1_v[...]
    ).astype(BF16)
    for d in range(zs):
        r.nsend[d * seq : (d + 1) * seq, :] = normed[:, d * wrap : (d + 1) * wrap]
    r.ncol[span(z, seq), :] = r.nsend[span(z, seq), :]
    pl.semaphore_wait(barrier, n - 1 + tpn - 1)

    arrived = {}
    for i, w in enumerate(order):
        for s in range(1, xs):
            arrived[WEIGHT, i, s] = send(
                w,
                r.wbuf.at[i, span(x, depth), :],
                WEIGHT,
                i * xs + s,
                device(z, lax.rem(x + s, xs), y, c),
            )
    for k in far_first:
        zz = zat(k)
        send(
            r.nsend.at[span(zz, seq)],
            r.ncol.at[span(z, seq)],
            NORMED,
            k,
            device(zz, x, y, c),
            z,
        )
    pieces = []
    if move:
        rows = r.dgate.shape[0]
        got.dgv = []
        for i, (src, dst) in enumerate(((r.dgate, r.dgv), (r.dup, r.duv))):
            for q in range(sides):
                for k in range(CORES):
                    core = twin_core if k else c
                    peer = lax.rem(y + q, sides) * CORES + core
                    count = PIECES if q else 1
                    size = rows // count
                    for j in range(count):
                        part = pl.ds(j * size, size)
                        a = src.at[part, span(peer, dff)]
                        b = dst.at[c, pl.ds(pl.multiple_of(y * rows + j * size, ROWS), size), :]
                        slot = ((i * sides + q) * CORES + k) * PIECES + j
                        if q:
                            pieces.append((a, b, slot, peer, i))
                        elif k:
                            arrived[MOVE, i, slot] = send(a, b, MOVE, slot, {"tp": peer})
                        else:
                            got.dgv.append(fetch(a, b))

    def move_pieces(count):
        for a, b, slot, peer, i in pieces[:count]:
            arrived[MOVE, i, slot] = send(a, b, MOVE, slot, {"tp": peer})
        del pieces[:count]

    def moved():
        for key, copy in arrived.items():
            if key[0] == MOVE:
                copy.wait_recv()

    move_pieces(AHEAD[0])

    got.ids.wait()
    got.weights.wait()
    got.mix.wait()
    eye = lax.broadcasted_iota(jnp.int32, (seq, lanes), 0) == lax.broadcasted_iota(
        jnp.int32, (seq, lanes), 1
    )
    ids, weights = r.ids_v[...], r.weights_v[...]
    rrows = r.rsend.shape[1]

    def to_row(col):
        return jnp.sum(jnp.where(eye, col, 0.0), axis=0, keepdims=True)

    def to_col(row):
        return jnp.sum(jnp.where(eye, row, 0.0), axis=1, keepdims=True)

    for d in range(n):
        r.rsend[d] = jnp.zeros((rrows, lanes), F32)
        for i in range(exp_local):
            r.rsend[d, i : i + 1, :seq] = jnp.sum(
                jnp.where(ids == d * exp_local + i, weights, 0.0), axis=0, keepdims=True
            )
    r.rrecv[me] = r.rsend[me]
    for s in range(1, n):
        peer = lax.rem(me + s, n)
        arrived[ROUTE, s] = send(
            r.rsend.at[peer], r.rrecv.at[me], ROUTE, s, {"ep": peer}
        )
    def fetch_rows(src, dst):
        return [
            fetch(src.at[span(t, cols), :], dst(t % CORES).at[span(t // CORES, cols), :])
            for t in range(tpn)
        ]

    got.sgv = fetch_rows(r.sg, lambda k: r.sgv.at[k]) + fetch_rows(r.su, lambda k: r.suv.at[k])
    got.sdv = [fetch(r.sd, r.sdv)]
    got.egv = []
    for e in range(exp_local):
        got.egv += fetch_rows(r.eg.at[e], lambda k: r.egv.at[k, e])
        got.egv += fetch_rows(r.eu.at[e], lambda k: r.euv.at[k, e])
    got.edv = [fetch(r.ed.at[e], r.edv.at[span(e, ff), :]) for e in range(exp_local)]
    got.ddv = fetch(r.ddown, r.ddv)
    if not move:
        got.dgv = fetch_rows(r.gatew, lambda k: r.dgv.at[k])
        got.dgv += fetch_rows(r.upw, lambda k: r.duv.at[k])

    for k in range(1, zs):
        landed(NORMED, zat(k), r.ncol.at[span(zat(k), seq)])
    for i in range(len(order)):
        got.w[i].wait()
        for s in range(1, xs):
            arrived[WEIGHT, i, s].wait_recv()
        r.psend[i] = jnp.dot(
            r.ncol[...], r.wbuf[i], preferred_element_type=F32
        ).astype(BF16)
        for k in far_first:
            zz = zat(k)
            send(
                r.psend.at[i, span(zz, seq)],
                r.precv.at[i, span(z, seq)],
                PROJ,
                i * zs + k,
                device(zz, x, y, c),
                i * zs + z,
            )

    def projected(i):
        total = r.psend[i, span(z, seq), :].astype(F32)
        for k in range(1, zs):
            zz = zat(k)
            landed(PROJ, i * zs + zz, r.precv.at[i, span(zz, seq)])
            total = total + r.precv[i, span(zz, seq), :].astype(F32)
        return total.astype(BF16).astype(F32)

    padded = ceil_to(seq, LANES)

    def turn(value, dst):
        if padded > seq:
            value = jnp.concatenate([value, jnp.zeros((padded - seq, mixw), F32)], axis=0)
        value = value.T
        for g in range(groups):
            dst[g] = value[:, g * ROWS : (g + 1) * ROWS]

    got.lb.wait()
    got.hg.wait()
    lb = r.lb_v[...]
    decay = lb + (1.0 - lb) * jax.nn.sigmoid(projected(0))
    query = projected(1)
    turn(decay, r.dturn)
    turn(query * decay, r.qturn)
    keyed = query * (1.0 - decay)
    for copy in states:
        copy.wait()

    def read_group(g, carry):
        qg = r.qturn[g]
        rows = []
        for b in range(ROWS):
            parts = [
                jnp.sum(
                    qg[h * hd : (h + 1) * hd, b : b + 1] * r.new_state[g * ROWS + b, h],
                    axis=0,
                    keepdims=True,
                )
                for h in range(heads)
            ]
            rows.append(jnp.concatenate(parts, axis=1))
        r.read[span(g, ROWS), :] = jnp.concatenate(rows, axis=0)
        return carry

    lax.fori_loop(0, groups, read_group, 0)

    def write_group(g, carry):
        dg = r.dturn[g]
        vg = r.vals[span(g, ROWS), :]
        for b in range(ROWS):
            for h in range(heads):
                at = slice(h * hd, (h + 1) * hd)
                vrow = vg[b : b + 1, at]
                old = r.new_state[g * ROWS + b, h]
                r.new_state[g * ROWS + b, h] = vrow + dg[at, b : b + 1] * (old - vrow)
        return carry

    values = projected(2)
    r.vals[...] = values
    read = r.read[...]
    parts = []
    for h in range(heads):
        at = slice(h * hd, (h + 1) * hd)
        part = read[:, at] + jnp.sum(keyed[:, at], axis=-1, keepdims=True) * values[:, at]
        parts.append(part * lax.rsqrt(jnp.mean(part * part, axis=-1, keepdims=True) + EPS))
    read = jnp.concatenate(parts, axis=1)
    head = (read * r.hg_v[...] * silu(projected(3))).astype(BF16)

    got.wout.wait()
    got.gain2.wait()
    for t in range(tpn):
        r.hsend[t] = jnp.dot(
            head, r.wout_v[:, t * cols : (t + 1) * cols], preferred_element_type=F32
        ).astype(BF16)
    for s in range(1, tpn):
        peer = lax.rem(tp + s, tpn)
        arrived[HEAD, s] = send(r.hsend.at[peer], r.hrecv.at[tp], HEAD, s, {"tp": peer})
    move_pieces(AHEAD[1])
    mine = span(tp, cols)
    total = r.tokens_v[:, mine].astype(F32) + r.hsend[tp].astype(F32)
    for s in range(1, tpn):
        arrived[HEAD, s].wait_recv()
        total = total + r.hrecv[lax.rem(tp + tpn - s, tpn)].astype(F32)
    r.resid[...] = total

    square = to_row(jnp.sum(total * total, axis=-1, keepdims=True))
    r.sqs[...] = jnp.broadcast_to(square, (ROWS, lanes))
    for s in range(1, tpn):
        arrived[SQUARE, s] = send(
            r.sqs, r.sqr.at[tp], SQUARE, s, {"tp": lax.rem(tp + s, tpn)}
        )
    def block(zz, xx, yy, cc):
        return r.rows.at[cc, span(zz * xs + xx, seq), span(yy, cols)]

    r.rows[c, span(me, seq), span(y, cols)] = (total * r.gain2_v[:, mine]).astype(BF16)
    own = block(z, x, y, c)
    for k in far_first:
        send(own, own, GATHER_Z, k, device(zat(k), x, y, c), z)

    offsets = [(a, b) for a in range(xs) for b in range(sides)]

    def plane(k, a, b):
        return block(zat(k), lax.rem(x + xs - a, xs), lax.rem(y + sides - b, sides), c)

    def place(k, a, b):
        return (k * xs + a) * sides + b

    def forward_twin(k, a, b):
        ref = plane(k, a, b)
        arrived[GATHER_C, k, a, b] = send(
            ref, ref, GATHER_C, place(k, a, b), device(z, x, y, twin_core)
        )

    def forward(k):
        ref = plane(k, 0, 0)
        for a, b in reversed(offsets[1:]):
            peer = device(z, lax.rem(x + a, xs), lax.rem(y + b, sides), c)
            arrived[GATHER_P, k, a, b] = send(ref, ref, GATHER_P, place(k, a, b), peer)
        forward_twin(k, 0, 0)

    forward(0)
    move_pieces(AHEAD[2])

    size = xs * seq
    def scale_out(k):
        square = r.sqs[:1]
        for s in range(1, tpn):
            arrived[SQUARE, s].wait_recv()
            square = square + r.sqr[lax.rem(tp + tpn - s, tpn)][:1]
        r.scr[me] = jnp.broadcast_to(lax.rsqrt(square / width + EPS), (ROWS, lanes))
        for s in range(1, n):
            send(r.scr.at[me], r.scr.at[me], SCALE, s, {"ep": lax.rem(me + s, n)}, me)

    def from_z(k):
        landed(GATHER_Z, zat(k), plane(k, 0, 0))
        forward(k)
        if k == zs - 1:
            move_pieces(len(pieces))

    def from_plane(k):
        for a, b in offsets[1:]:
            arrived[GATHER_P, k, a, b].wait_recv()
            forward_twin(k, a, b)

    def first_half(k):
        if k == 0:
            for copy in got.egv:
                copy.wait()
        lhs = r.rows[c, span(zat(k), size), :]
        for i in range(exp_local):
            for j, ref in enumerate((r.egv, r.euv)):
                r.acc[2 * i + j, k] = jnp.dot(lhs, ref[c, i], preferred_element_type=F32)

    def column(ref, k, row):
        return jnp.concatenate(
            [to_col(ref[zat(k) * xs + i][row : row + 1]) for i in range(xs)], axis=0
        )

    def shared_expert():
        for copy in got.sgv + got.sdv:
            copy.wait()
        pre = [
            sum(
                jnp.dot(r.rows[k, span(me, seq), :], ref[k], preferred_element_type=F32)
                for k in range(CORES)
            )
            for ref in (r.sgv, r.suv)
        ]
        own_scale = to_col(r.scr[me][:1])
        hidden = (silu(own_scale * pre[0]) * (own_scale * pre[1])).astype(BF16)
        for t in range(tpn):
            r.shared[t] = jnp.dot(
                hidden, r.sdv[:, t * cols : (t + 1) * cols], preferred_element_type=F32
            )

    def partial(k, yy, cc):
        t = yy * CORES + cc
        value = jnp.dot(r.hid[k], r.edv[:, span(t, cols)], preferred_element_type=F32)
        if k == 0:
            r.wide[...] = value
            r.wide[span(x, seq), :] = r.wide[span(x, seq), :] + r.shared[t]
            value = r.wide[...]
        return value

    def second_half(k):
        for a, b in offsets:
            arrived[GATHER_C, k, a, b].wait_recv()
        if k == 0:
            for s in range(1, n):
                arrived[ROUTE, s].wait_recv()
        for i in range(xs):
            if k or i:
                e = zat(k) * xs + lax.rem(x + i, xs)
                landed(SCALE, e, r.scr.at[e])
        scale = column(r.scr, k, 0)
        lhs = r.rows[twin_core, span(zat(k), size), :]
        for i in range(exp_local):
            gate, up = [
                scale
                * (
                    r.acc[2 * i + j, k]
                    + jnp.dot(lhs, ref[twin_core, i], preferred_element_type=F32)
                )
                for j, ref in enumerate((r.egv, r.euv))
            ]
            share = column(r.rrecv, k, i)
            r.hid[k, :, i * ff : (i + 1) * ff] = (silu(gate) * up * share).astype(BF16)

    def dense_hidden(k):
        if k == 0:
            for copy in got.dgv:
                copy.wait()
            moved()
        scale = column(r.scr, k, 0)
        gate, up = [
            scale
            * sum(
                jnp.dot(r.rows[i, span(zat(k), size), :], ref[i], preferred_element_type=F32)
                for i in range(CORES)
            )
            for ref in (r.dgv, r.duv)
        ]
        r.dhid[k, tp] = (silu(gate) * up).astype(BF16)
        ref = r.dhid.at[k, tp]
        for q in range(1, sides):
            peer = device(z, x, lax.rem(y + q, sides), c)
            arrived[HIDDEN_Y, k, q] = send(ref, ref, HIDDEN_Y, k * sides + q, peer)
        arrived[HIDDEN_C, k, 0] = send(ref, ref, HIDDEN_C, k * sides, device(z, x, y, twin_core))

    def down(k):
        if k == 0:
            for copy in got.edv:
                copy.wait()
            shared_expert()
        for q in range(sides):
            r.part[k * sides + q] = partial(k, lax.rem(y + q, sides), twin_core).astype(BF16)
        for q in [*range(1, sides), 0]:
            slot = k * sides + q
            arrived[SUM_C, k, q] = send(
                r.part.at[slot], r.crecv.at[slot], SUM_C, slot, device(z, x, y, twin_core)
            )

    def hidden_on(k):
        for q in range(1, sides):
            arrived[HIDDEN_Y, k, q].wait_recv()
            ref = r.dhid.at[k, lax.rem(y + sides - q, sides) * CORES + c]
            arrived[HIDDEN_C, k, q] = send(
                ref, ref, HIDDEN_C, k * sides + q, device(z, x, y, twin_core)
            )

    def from_twin(k):
        values = [partial(k, lax.rem(y + q, sides), c) for q in range(sides)]
        for q in [*range(1, sides), 0]:
            slot = k * sides + q
            arrived[SUM_C, k, q].wait_recv()
            value = values[q] + r.crecv[slot].astype(F32)
            if q == 0:
                r.keep[k] = value
                continue
            r.ysend[slot] = value.astype(BF16)
            for j in range(xs):
                sum_out(k, j, q, r.ysend.at[slot, span(lax.rem(x + j, xs), seq)])

    def sum_out(k, j, q, ref):
        peer = device(z, lax.rem(x + j, xs), lax.rem(y + q, sides), c)
        at = place(k, j, q)
        arrived[SUM_P, k, j, q] = send(ref, r.plane_sums.at[at], SUM_P, at, peer)

    def add_dense(k):
        for q in range(sides):
            arrived[HIDDEN_C, k, q].wait_recv()
        if k == 0:
            got.ddv.wait()
        dense = sum(
            jnp.dot(
                r.dhid[k, t], r.ddv[t * dff : (t + 1) * dff, :], preferred_element_type=F32
            )
            for t in range(tpn)
        )
        r.keep[k] = r.keep[k] + jax.nn.sigmoid(r.mix_v[...]) * dense
        for j in range(1, xs):
            slot = k * sides
            rows_at = span(lax.rem(x + j, xs), seq)
            r.ysend[slot, rows_at, :] = r.keep[k, rows_at, :].astype(BF16)
            sum_out(k, j, 0, r.ysend.at[slot, rows_at])

    def from_sums(k):
        value = r.keep[k, span(x, seq), :]
        for j, q in offsets[1:]:
            arrived[SUM_P, k, j, q].wait_recv()
            value = value + r.plane_sums[place(k, j, q)].astype(F32)
        if k == 0:
            r.resid[...] = r.resid[...] + value
        else:
            r.zsend[k] = value.astype(BF16)
            send(r.zsend.at[k], r.zrecv.at[z], SUM_Z, k, device(zat(k), x, y, c), z)

    def write_state(k):
        lax.fori_loop(0, groups, write_group, 0)

    kinds = (
        from_z,
        from_plane,
        first_half,
        second_half,
        down,
        dense_hidden,
        from_twin,
        hidden_on,
        add_dense,
        from_sums,
        scale_out,
        write_state,
    )
    for kind, k in schedule(zs):
        step = kinds[kind]
        step(k)

    final = r.resid[...]
    for k in range(1, zs):
        landed(SUM_Z, zat(k), r.zrecv.at[zat(k)])
        final = final + r.zrecv[zat(k)].astype(F32)
    r.out[...] = final.astype(BF16)

    for copy in waiting:
        copy.wait_send()


def place_kernel(held, held_state, out, new_state, sems):
    parts = [pl.ds(g * ROWS, ROWS) for g in range(held_state.shape[0] // ROWS)]
    moves = [(held_state.at[p], new_state.at[p]) for p in parts] + [(held, out)]
    copies = [pltpu.make_async_copy(*move, sems.at[k]) for k, move in enumerate(moves)]
    for copy in copies:
        copy.start()
    for copy in copies:
        copy.wait()


def local(
    tokens,
    state,
    norm_gain,
    w_query,
    w_forget,
    w_input,
    w_outgate,
    lower_bound,
    head_gain,
    w_output,
    ffn_gain,
    route_ids,
    route_weight,
    expert_gate,
    expert_up,
    expert_down,
    shared_gate,
    shared_up,
    shared_down,
    dense_gate,
    dense_up,
    dense_down,
    dense_mix,
):
    n = lax.axis_size("ep")
    tpn = lax.axis_size("tp")
    sides = tpn // CORES
    zs = n // sides
    seq, width = tokens.shape
    depth, mixw = w_query.shape
    heads, hd = state.shape[1:3]
    cols = width // tpn
    half = sides * cols
    exp_local, _, ff = expert_gate.shape
    sff = shared_gate.shape[1]
    dff = dense_gate.shape[1] // tpn
    lanes = ceil_to(seq, LANES)
    rrows = ceil_to(exp_local, ROWS)
    groups = seq // ROWS
    move = dff % LANES == 0
    sds = jax.ShapeDtypeStruct
    VM, ANY = pltpu.VMEM, pl.ANY

    ins = dict(
        tokens=tokens,
        state=state,
        gain1=norm_gain[None, :],
        wq=w_query,
        wf=w_forget,
        wi=w_input,
        wo=w_outgate,
        lb=lower_bound[None, :],
        hg=head_gain[None, :],
        wout=w_output,
        gain2=ffn_gain[None, :],
        ids=route_ids.T,
        weights=route_weight.T,
        eg=expert_gate,
        eu=expert_up,
        ed=expert_down,
        sg=shared_gate,
        su=shared_up,
        sd=shared_down,
        mix=dense_mix[None, :],
        ddown=dense_down,
    )
    if move:
        ins.update(dgate=dense_gate, dup=dense_up)
    else:
        gate_w, up_w = [
            lax.all_to_all(w, "tp", split_axis=1, concat_axis=0, tiled=True)
            for w in (dense_gate, dense_up)
        ]
        ins.update(gatew=gate_w, upw=up_w)
    outs = dict(out=sds((seq, cols), BF16), new_state=sds(state.shape, F32))
    hops = zs * sides * sides
    size = sides * seq
    scratch = dict(
        tokens_v=VM((seq, width), BF16),
        gain1_v=VM((1, width), F32),
        gain2_v=VM((1, width), F32),
        lb_v=VM((1, mixw), F32),
        hg_v=VM((1, mixw), F32),
        mix_v=VM((1, cols), F32),
        ids_v=VM(route_ids.shape[::-1], jnp.int32),
        weights_v=VM(route_weight.shape[::-1], F32),
        wout_v=VM((mixw, width), BF16),
        nsend=VM((zs * seq, sides * depth), BF16),
        ncol=VM((zs * seq, sides * depth), BF16),
        wbuf=VM((4, sides * depth, mixw), BF16),
        psend=VM((4, zs * seq, mixw), BF16),
        precv=VM((4, zs * seq, mixw), BF16),
        dturn=VM((groups, mixw, ROWS), F32),
        qturn=VM((groups, mixw, ROWS), F32),
        vals=VM((seq, mixw), F32),
        read=VM((seq, mixw), F32),
        rsend=VM((n, rrows, lanes), F32),
        rrecv=VM((n, rrows, lanes), F32),
        hsend=VM((tpn, seq, cols), BF16),
        hrecv=VM((tpn, seq, cols), BF16),
        resid=VM((seq, cols), F32),
        rows=VM((CORES, n * seq, half), BF16),
        sqs=VM((ROWS, lanes), F32),
        sqr=VM((tpn, ROWS, lanes), F32),
        scr=VM((n, ROWS, lanes), F32),
        egv=VM((CORES, exp_local, half, ff), BF16),
        euv=VM((CORES, exp_local, half, ff), BF16),
        edv=VM((exp_local * ff, width), BF16),
        sgv=VM((CORES, half, sff), BF16),
        suv=VM((CORES, half, sff), BF16),
        sdv=VM((sff, width), BF16),
        dgv=VM((CORES, half, dff), BF16),
        duv=VM((CORES, half, dff), BF16),
        ddv=VM(dense_down.shape, BF16),
        acc=VM((2 * exp_local, zs, size, ff), F32),
        hid=VM((zs, size, exp_local * ff), BF16),
        dhid=VM((zs, tpn, size, dff), BF16),
        wide=VM((size, cols), F32),
        part=VM((zs * sides, size, cols), BF16),
        crecv=VM((zs * sides, size, cols), BF16),
        ysend=VM((zs * sides, size, cols), BF16),
        plane_sums=VM((hops, seq, cols), BF16),
        keep=VM((zs, size, cols), F32),
        zsend=VM((zs, seq, cols), BF16),
        zrecv=VM((zs, seq, cols), BF16),
        shared=VM((tpn, seq, cols), F32),
        local=pltpu.SemaphoreType.DMA((64 + groups + 8 * exp_local * tpn,)),
    )
    counts = {
        WEIGHT: 4 * sides,
        NORMED: zs,
        MOVE: 2 * tpn * PIECES,
        ROUTE: n,
        HIDDEN_Y: zs * sides,
        HIDDEN_C: zs * sides,
        PROJ: 4 * zs,
        HEAD: tpn,
        GATHER_Z: zs,
        GATHER_P: hops,
        GATHER_C: hops,
        SQUARE: tpn,
        SCALE: n,
        SUM_C: zs * sides,
        SUM_P: hops,
        SUM_Z: zs,
    }
    names = [*ins, *outs, *scratch]
    sems = [pltpu.SemaphoreType.DMA((counts[k],)) for k in range(len(counts)) for _ in range(2)]
    held = pl.pallas_call(
        functools.partial(layer_kernel, n, tpn, move, names),
        out_shape=tuple(VM(out.shape, out.dtype) for out in outs.values()),
        in_specs=[pl.BlockSpec(memory_space=ANY) for _ in ins],
        out_specs=(pl.BlockSpec(memory_space=VM),) * 2,
        scratch_shapes=list(scratch.values()) + sems,
        compiler_params=pltpu.CompilerParams(
            collective_id=0, has_side_effects=True, vmem_limit_bytes=VMEM_BYTES
        ),
    )(*ins.values())
    return pl.pallas_call(
        place_kernel,
        out_shape=tuple(outs.values()),
        in_specs=[pl.BlockSpec(memory_space=VM)] * 2,
        out_specs=(pl.BlockSpec(memory_space=ANY),) * 2,
        scratch_shapes=[pltpu.SemaphoreType.DMA((groups + 1,))],
        compiler_params=pltpu.CompilerParams(vmem_limit_bytes=PLACE_BYTES),
    )(*[pltpu.with_memory_space_constraint(a, VM) for a in held])


def solution(mesh):
    placed = (
        P("ep", None),
        P("ep", "tp", None, None),
        P(),
        P("ep", "tp"),
        P("ep", "tp"),
        P("ep", "tp"),
        P("ep", "tp"),
        P("tp"),
        P("tp"),
        P("tp", None),
        P(),
        P("ep", None),
        P("ep", None),
        P("ep", None, "tp"),
        P("ep", None, "tp"),
        P("ep", "tp", None),
        P(None, "tp"),
        P(None, "tp"),
        P("tp", None),
        P("tp", "ep"),
        P("tp", "ep"),
        P("ep", "tp"),
        P("tp"),
    )
    return jax.shard_map(
        local,
        mesh=mesh,
        in_specs=placed,
        out_specs=(P("ep", "tp"), P("ep", "tp", None, None)),
        check_vma=False,
    )
```

```python
import functools
import types

import jax
import jax.numpy as jnp
from jax import lax
from jax.experimental import pallas as pl
from jax.experimental.pallas import tpu as pltpu
from jax.sharding import PartitionSpec as P

EPS = 1e-06
LANES = 128
CORES = 2
ROWS = 8
F32 = jnp.float32
BF16 = jnp.bfloat16
PIECES = 4
AHEAD = (12, 2, 2)
MOVED_AT = 10.0
PLACE_BYTES = 1024 * 1024
VMEM_BYTES = 52 * 1024 * 1024
(
    WEIGHT,
    NORMED,
    MOVE,
    ROUTE,
    HIDDEN_Y,
    HIDDEN_C,
    PROJ,
    HEAD,
    GATHER_Z,
    GATHER_P,
    GATHER_C,
    SQUARE,
    SCALE,
    SUM_C,
    SUM_P,
    SUM_Z,
) = range(16)


def span(index, size):
    if isinstance(index, int):
        return pl.ds(index * size, size)
    return pl.ds(pl.multiple_of(index * size, size), size)


def ceil_to(value, step):
    return -(-value // step) * step


def silu(v):
    return v * jax.nn.sigmoid(v)


def schedule(zs):
    Z, PLANE, HALF, SECOND, DOWN, DENSE, TWIN, HIDDEN, ADD, SUMS, SCALES, STATE = range(12)
    cost = (0.05, 0.08, 0.4, 0.55, 0.35, 0.55, 0.5, 0.05, 0.35, 0.05, 0.1, 2.1)
    relays = (Z, PLANE, SCALES, HIDDEN)
    after = {(STATE, 0): [], (SCALES, 0): [(None, 2.5)]}
    for k in range(zs):
        after[Z, k] = [(None, 2.8 + 1.6 * k if k else 0.0)]
        after[PLANE, k] = [((Z, k), 3.2)]
        after[HALF, k] = [((PLANE, k), 0.0)]
        after[SECOND, k] = [((PLANE, k), 1.4), ((HALF, k), 0.0), ((SCALES, 0), 2.5)]
        after[DOWN, k] = [((SECOND, k), 0.0), ((Z, zs - 1), 0.0)]
        after[DENSE, k] = [((SECOND, k), 0.0), (None, MOVED_AT)]
        after[TWIN, k] = [((DOWN, k), 1.4)]
        after[HIDDEN, k] = [((DENSE, k), 4.0)]
        after[ADD, k] = [((TWIN, k), 0.0), ((HIDDEN, k), 1.3)]
        after[SUMS, k] = [((TWIN, k), 3.6), ((ADD, k), 2.9)]
    done, now, order = {(Z, 0): 0.0, None: 0.0}, 0.0, []
    del after[Z, 0]
    while after:
        ready = {
            step: max([done[need] + wait for need, wait in needs] or [0.0])
            for step, needs in after.items()
            if all(need in done for need, _ in needs)
        }
        now = max(now, min(ready.values()))
        step = min(
            (step for step, at in ready.items() if at <= now),
            key=lambda step: (step[0] not in relays, step[0] == STATE, step[0] in (ADD, TWIN), -step[0], step[1]),
        )
        now += cost[step[0]] + (0.8 if step == (DOWN, 0) else 0.0)
        done[step] = now
        order.append(step)
        del after[step]
    return order


def layer_kernel(n, tpn, move, names, *refs):
    sems = refs[len(names) :]
    r = types.SimpleNamespace(**dict(zip(names, refs)))
    me, tp = lax.axis_index("ep"), lax.axis_index("tp")
    sides = tpn // CORES
    xs = sides
    zs = n // xs
    z, x = lax.div(me, xs), lax.rem(me, xs)
    y, c = lax.div(tp, CORES), lax.rem(tp, CORES)
    twin_core = CORES - 1 - c
    seq, width = r.tokens.shape
    cols = width // tpn
    depth, mixw = r.wq.shape
    exp_local, _, ff = r.eg.shape
    sff = r.sg.shape[1]
    dff = r.dgv.shape[2]
    heads, hd = r.state.shape[1:3]
    wrap = xs * depth
    lanes = r.sqs.shape[1]
    half = sides * cols

    def device(zz, xx, yy, cc):
        return {"ep": zz * xs + xx, "tp": yy * CORES + cc}

    waiting = []

    def send(src, dst, kind, slot, peer, landing=None):
        copy = pltpu.make_async_remote_copy(
            src_ref=src,
            dst_ref=dst,
            send_sem=sems[2 * kind].at[slot],
            recv_sem=sems[2 * kind + 1].at[slot if landing is None else landing],
            device_id=peer,
            device_id_type=pl.DeviceIdType.MESH,
        )
        copy.start()
        waiting.append(copy)
        return copy

    def landed(kind, slot, ref):
        pltpu.make_async_remote_copy(
            src_ref=ref,
            dst_ref=ref,
            send_sem=sems[2 * kind].at[slot],
            recv_sem=sems[2 * kind + 1].at[slot],
            device_id=device(z, x, y, twin_core),
            device_id_type=pl.DeviceIdType.MESH,
        ).wait_recv()

    high = lax.div(2 * z, zs)
    near = z * (1 - high) + (zs - 1 - z) * high

    def zat(k):
        if k == 0:
            return z
        place = k - 1 + lax.div(zs + k - 1 - near, zs)
        return place * (1 - high) + (zs - 1 - place) * high

    far_first = range(zs - 1, 0, -1)
    used = [0]

    def fetch(src, dst):
        copy = pltpu.make_async_copy(src, dst, r.local.at[used[0]])
        used[0] += 1
        copy.start()
        return copy

    got = types.SimpleNamespace()
    got.tokens = fetch(r.tokens, r.tokens_v)
    got.gain1 = fetch(r.gain1, r.gain1_v)
    order = (r.wf, r.wq, r.wi, r.wo)
    got.w = [fetch(w, r.wbuf.at[i, span(x, depth), :]) for i, w in enumerate(order)]
    got.lb = fetch(r.lb, r.lb_v)
    got.hg = fetch(r.hg, r.hg_v)
    got.mix = fetch(r.mix, r.mix_v)
    got.ids = fetch(r.ids, r.ids_v)
    got.weights = fetch(r.weights, r.weights_v)
    groups = seq // ROWS
    states = [
        fetch(r.state.at[pl.ds(g * ROWS, ROWS)], r.new_state.at[pl.ds(g * ROWS, ROWS)])
        for g in range(groups)
    ]
    got.wout = fetch(r.wout, r.wout_v)
    got.gain2 = fetch(r.gain2, r.gain2_v)

    barrier = pltpu.get_barrier_semaphore()
    for s in range(1, tpn):
        pl.semaphore_signal(
            barrier,
            inc=1,
            device_id={"tp": lax.rem(tp + s, tpn)},
            device_id_type=pl.DeviceIdType.MESH,
        )
    for s in range(1, n):
        pl.semaphore_signal(
            barrier,
            inc=1,
            device_id={"ep": lax.rem(me + s, n)},
            device_id_type=pl.DeviceIdType.MESH,
        )
    got.tokens.wait()
    got.gain1.wait()
    t32 = r.tokens_v[...].astype(F32)
    normed = (
        t32 * lax.rsqrt(jnp.mean(t32 * t32, axis=-1, keepdims=True) + EPS) * r.gain1_v[...]
    ).astype(BF16)
    for d in range(zs):
        r.nsend[d * seq : (d + 1) * seq, :] = normed[:, d * wrap : (d + 1) * wrap]
    r.ncol[span(z, seq), :] = r.nsend[span(z, seq), :]
    pl.semaphore_wait(barrier, n - 1 + tpn - 1)

    arrived = {}
    for i, w in enumerate(order):
        for s in range(1, xs):
            arrived[WEIGHT, i, s] = send(
                w,
                r.wbuf.at[i, span(x, depth), :],
                WEIGHT,
                i * xs + s,
                device(z, lax.rem(x + s, xs), y, c),
            )
    for k in far_first:
        zz = zat(k)
        send(
            r.nsend.at[span(zz, seq)],
            r.ncol.at[span(z, seq)],
            NORMED,
            k,
            device(zz, x, y, c),
            z,
        )
    pieces = []
    if move:
        rows = r.dgate.shape[0]
        got.dgv = []
        for i, (src, dst) in enumerate(((r.dgate, r.dgv), (r.dup, r.duv))):
            for q in range(sides):
                for k in range(CORES):
                    core = twin_core if k else c
                    peer = lax.rem(y + q, sides) * CORES + core
                    count = PIECES if q else 1
                    size = rows // count
                    for j in range(count):
                        part = pl.ds(j * size, size)
                        a = src.at[part, span(peer, dff)]
                        b = dst.at[c, pl.ds(pl.multiple_of(y * rows + j * size, ROWS), size), :]
                        slot = ((i * sides + q) * CORES + k) * PIECES + j
                        if q:
                            pieces.append((a, b, slot, peer, i))
                        elif k:
                            arrived[MOVE, i, slot] = send(a, b, MOVE, slot, {"tp": peer})
                        else:
                            got.dgv.append(fetch(a, b))

    def move_pieces(count):
        for a, b, slot, peer, i in pieces[:count]:
            arrived[MOVE, i, slot] = send(a, b, MOVE, slot, {"tp": peer})
        del pieces[:count]

    def moved():
        for key, copy in arrived.items():
            if key[0] == MOVE:
                copy.wait_recv()

    move_pieces(AHEAD[0])

    got.ids.wait()
    got.weights.wait()
    got.mix.wait()
    eye = lax.broadcasted_iota(jnp.int32, (seq, lanes), 0) == lax.broadcasted_iota(
        jnp.int32, (seq, lanes), 1
    )
    ids, weights = r.ids_v[...], r.weights_v[...]
    rrows = r.rsend.shape[1]

    def to_row(col):
        return jnp.sum(jnp.where(eye, col, 0.0), axis=0, keepdims=True)

    def to_col(row):
        return jnp.sum(jnp.where(eye, row, 0.0), axis=1, keepdims=True)

    for d in range(n):
        r.rsend[d] = jnp.zeros((rrows, lanes), F32)
        for i in range(exp_local):
            r.rsend[d, i : i + 1, :seq] = jnp.sum(
                jnp.where(ids == d * exp_local + i, weights, 0.0), axis=0, keepdims=True
            )
    r.rrecv[me] = r.rsend[me]
    for s in range(1, n):
        peer = lax.rem(me + s, n)
        arrived[ROUTE, s] = send(
            r.rsend.at[peer], r.rrecv.at[me], ROUTE, s, {"ep": peer}
        )
    def fetch_rows(src, dst):
        return [
            fetch(src.at[span(t, cols), :], dst(t % CORES).at[span(t // CORES, cols), :])
            for t in range(tpn)
        ]

    got.sgv = fetch_rows(r.sg, lambda k: r.sgv.at[k]) + fetch_rows(r.su, lambda k: r.suv.at[k])
    got.sdv = [fetch(r.sd, r.sdv)]
    got.egv = []
    for e in range(exp_local):
        got.egv += fetch_rows(r.eg.at[e], lambda k: r.egv.at[k, e])
        got.egv += fetch_rows(r.eu.at[e], lambda k: r.euv.at[k, e])
    got.edv = [fetch(r.ed.at[e], r.edv.at[span(e, ff), :]) for e in range(exp_local)]
    got.ddv = fetch(r.ddown, r.ddv)
    if not move:
        got.dgv = fetch_rows(r.gatew, lambda k: r.dgv.at[k])
        got.dgv += fetch_rows(r.upw, lambda k: r.duv.at[k])

    for k in range(1, zs):
        landed(NORMED, zat(k), r.ncol.at[span(zat(k), seq)])
    for i in range(len(order)):
        got.w[i].wait()
        for s in range(1, xs):
            arrived[WEIGHT, i, s].wait_recv()
        r.psend[i] = jnp.dot(
            r.ncol[...], r.wbuf[i], preferred_element_type=F32
        ).astype(BF16)
        for k in far_first:
            zz = zat(k)
            send(
                r.psend.at[i, span(zz, seq)],
                r.precv.at[i, span(z, seq)],
                PROJ,
                i * zs + k,
                device(zz, x, y, c),
                i * zs + z,
            )

    def projected(i):
        total = r.psend[i, span(z, seq), :].astype(F32)
        for k in range(1, zs):
            zz = zat(k)
            landed(PROJ, i * zs + zz, r.precv.at[i, span(zz, seq)])
            total = total + r.precv[i, span(zz, seq), :].astype(F32)
        return total.astype(BF16).astype(F32)

    padded = ceil_to(seq, LANES)

    def turn(value, dst):
        if padded > seq:
            value = jnp.concatenate([value, jnp.zeros((padded - seq, mixw), F32)], axis=0)
        value = value.T
        for g in range(groups):
            dst[g] = value[:, g * ROWS : (g + 1) * ROWS]

    got.lb.wait()
    got.hg.wait()
    lb = r.lb_v[...]
    decay = lb + (1.0 - lb) * jax.nn.sigmoid(projected(0))
    query = projected(1)
    turn(decay, r.dturn)
    turn(query * decay, r.qturn)
    keyed = query * (1.0 - decay)
    for copy in states:
        copy.wait()

    def read_group(g, carry):
        qg = r.qturn[g]
        rows = []
        for b in range(ROWS):
            parts = [
                jnp.sum(
                    qg[h * hd : (h + 1) * hd, b : b + 1] * r.new_state[g * ROWS + b, h],
                    axis=0,
                    keepdims=True,
                )
                for h in range(heads)
            ]
            rows.append(jnp.concatenate(parts, axis=1))
        r.read[span(g, ROWS), :] = jnp.concatenate(rows, axis=0)
        return carry

    lax.fori_loop(0, groups, read_group, 0)

    def write_group(g, carry):
        dg = r.dturn[g]
        vg = r.vals[span(g, ROWS), :]
        for b in range(ROWS):
            for h in range(heads):
                at = slice(h * hd, (h + 1) * hd)
                vrow = vg[b : b + 1, at]
                old = r.new_state[g * ROWS + b, h]
                r.new_state[g * ROWS + b, h] = vrow + dg[at, b : b + 1] * (old - vrow)
        return carry

    values = projected(2)
    r.vals[...] = values
    read = r.read[...]
    parts = []
    for h in range(heads):
        at = slice(h * hd, (h + 1) * hd)
        part = read[:, at] + jnp.sum(keyed[:, at], axis=-1, keepdims=True) * values[:, at]
        parts.append(part * lax.rsqrt(jnp.mean(part * part, axis=-1, keepdims=True) + EPS))
    read = jnp.concatenate(parts, axis=1)
    head = (read * r.hg_v[...] * silu(projected(3))).astype(BF16)

    got.wout.wait()
    got.gain2.wait()
    for t in range(tpn):
        r.hsend[t] = jnp.dot(
            head, r.wout_v[:, t * cols : (t + 1) * cols], preferred_element_type=F32
        ).astype(BF16)
    for s in range(1, tpn):
        peer = lax.rem(tp + s, tpn)
        arrived[HEAD, s] = send(r.hsend.at[peer], r.hrecv.at[tp], HEAD, s, {"tp": peer})
    move_pieces(AHEAD[1])
    mine = span(tp, cols)
    total = r.tokens_v[:, mine].astype(F32) + r.hsend[tp].astype(F32)
    for s in range(1, tpn):
        arrived[HEAD, s].wait_recv()
        total = total + r.hrecv[lax.rem(tp + tpn - s, tpn)].astype(F32)
    r.resid[...] = total

    square = to_row(jnp.sum(total * total, axis=-1, keepdims=True))
    r.sqs[...] = jnp.broadcast_to(square, (ROWS, lanes))
    for s in range(1, tpn):
        arrived[SQUARE, s] = send(
            r.sqs, r.sqr.at[tp], SQUARE, s, {"tp": lax.rem(tp + s, tpn)}
        )
    def block(zz, xx, yy, cc):
        return r.rows.at[cc, span(zz * xs + xx, seq), span(yy, cols)]

    r.rows[c, span(me, seq), span(y, cols)] = (total * r.gain2_v[:, mine]).astype(BF16)
    own = block(z, x, y, c)
    for k in far_first:
        send(own, own, GATHER_Z, k, device(zat(k), x, y, c), z)

    offsets = [(a, b) for a in range(xs) for b in range(sides)]

    def plane(k, a, b):
        return block(zat(k), lax.rem(x + xs - a, xs), lax.rem(y + sides - b, sides), c)

    def place(k, a, b):
        return (k * xs + a) * sides + b

    def forward_twin(k, a, b):
        ref = plane(k, a, b)
        arrived[GATHER_C, k, a, b] = send(
            ref, ref, GATHER_C, place(k, a, b), device(z, x, y, twin_core)
        )

    def forward(k):
        ref = plane(k, 0, 0)
        for a, b in reversed(offsets[1:]):
            peer = device(z, lax.rem(x + a, xs), lax.rem(y + b, sides), c)
            arrived[GATHER_P, k, a, b] = send(ref, ref, GATHER_P, place(k, a, b), peer)
        forward_twin(k, 0, 0)

    forward(0)
    move_pieces(AHEAD[2])

    size = xs * seq
    def scale_out(k):
        square = r.sqs[:1]
        for s in range(1, tpn):
            arrived[SQUARE, s].wait_recv()
            square = square + r.sqr[lax.rem(tp + tpn - s, tpn)][:1]
        r.scr[me] = jnp.broadcast_to(lax.rsqrt(square / width + EPS), (ROWS, lanes))
        for s in range(1, n):
            send(r.scr.at[me], r.scr.at[me], SCALE, s, {"ep": lax.rem(me + s, n)}, me)

    def from_z(k):
        landed(GATHER_Z, zat(k), plane(k, 0, 0))
        forward(k)
        if k == zs - 1:
            move_pieces(len(pieces))

    def from_plane(k):
        for a, b in offsets[1:]:
            arrived[GATHER_P, k, a, b].wait_recv()
            forward_twin(k, a, b)

    def first_half(k):
        if k == 0:
            for copy in got.egv:
                copy.wait()
        lhs = r.rows[c, span(zat(k), size), :]
        for i in range(exp_local):
            for j, ref in enumerate((r.egv, r.euv)):
                r.acc[2 * i + j, k] = jnp.dot(lhs, ref[c, i], preferred_element_type=F32)

    def column(ref, k, row):
        return jnp.concatenate(
            [to_col(ref[zat(k) * xs + i][row : row + 1]) for i in range(xs)], axis=0
        )

    def shared_expert():
        for copy in got.sgv + got.sdv:
            copy.wait()
        pre = [
            sum(
                jnp.dot(r.rows[k, span(me, seq), :], ref[k], preferred_element_type=F32)
                for k in range(CORES)
            )
            for ref in (r.sgv, r.suv)
        ]
        own_scale = to_col(r.scr[me][:1])
        hidden = (silu(own_scale * pre[0]) * (own_scale * pre[1])).astype(BF16)
        for t in range(tpn):
            r.shared[t] = jnp.dot(
                hidden, r.sdv[:, t * cols : (t + 1) * cols], preferred_element_type=F32
            )

    def partial(k, yy, cc):
        t = yy * CORES + cc
        value = jnp.dot(r.hid[k], r.edv[:, span(t, cols)], preferred_element_type=F32)
        if k == 0:
            r.wide[...] = value
            r.wide[span(x, seq), :] = r.wide[span(x, seq), :] + r.shared[t]
            value = r.wide[...]
        return value

    def second_half(k):
        for a, b in offsets:
            arrived[GATHER_C, k, a, b].wait_recv()
        if k == 0:
            for s in range(1, n):
                arrived[ROUTE, s].wait_recv()
        for i in range(xs):
            if k or i:
                e = zat(k) * xs + lax.rem(x + i, xs)
                landed(SCALE, e, r.scr.at[e])
        scale = column(r.scr, k, 0)
        lhs = r.rows[twin_core, span(zat(k), size), :]
        for i in range(exp_local):
            gate, up = [
                scale
                * (
                    r.acc[2 * i + j, k]
                    + jnp.dot(lhs, ref[twin_core, i], preferred_element_type=F32)
                )
                for j, ref in enumerate((r.egv, r.euv))
            ]
            share = column(r.rrecv, k, i)
            r.hid[k, :, i * ff : (i + 1) * ff] = (silu(gate) * up * share).astype(BF16)

    def dense_hidden(k):
        if k == 0:
            for copy in got.dgv:
                copy.wait()
            moved()
        scale = column(r.scr, k, 0)
        gate, up = [
            scale
            * sum(
                jnp.dot(r.rows[i, span(zat(k), size), :], ref[i], preferred_element_type=F32)
                for i in range(CORES)
            )
            for ref in (r.dgv, r.duv)
        ]
        r.dhid[k, tp] = (silu(gate) * up).astype(BF16)
        ref = r.dhid.at[k, tp]
        for q in range(1, sides):
            peer = device(z, x, lax.rem(y + q, sides), c)
            arrived[HIDDEN_Y, k, q] = send(ref, ref, HIDDEN_Y, k * sides + q, peer)
        arrived[HIDDEN_C, k, 0] = send(ref, ref, HIDDEN_C, k * sides, device(z, x, y, twin_core))

    def down(k):
        if k == 0:
            for copy in got.edv:
                copy.wait()
            shared_expert()
        for q in range(sides):
            r.part[k * sides + q] = partial(k, lax.rem(y + q, sides), twin_core).astype(BF16)
        for q in [*range(1, sides), 0]:
            slot = k * sides + q
            arrived[SUM_C, k, q] = send(
                r.part.at[slot], r.crecv.at[slot], SUM_C, slot, device(z, x, y, twin_core)
            )

    def hidden_on(k):
        for q in range(1, sides):
            arrived[HIDDEN_Y, k, q].wait_recv()
            ref = r.dhid.at[k, lax.rem(y + sides - q, sides) * CORES + c]
            arrived[HIDDEN_C, k, q] = send(
                ref, ref, HIDDEN_C, k * sides + q, device(z, x, y, twin_core)
            )

    def from_twin(k):
        values = [partial(k, lax.rem(y + q, sides), c) for q in range(sides)]
        for q in [*range(1, sides), 0]:
            slot = k * sides + q
            arrived[SUM_C, k, q].wait_recv()
            value = values[q] + r.crecv[slot].astype(F32)
            if q == 0:
                r.keep[k] = value
                continue
            r.ysend[slot] = value.astype(BF16)
            for j in range(xs):
                sum_out(k, j, q, r.ysend.at[slot, span(lax.rem(x + j, xs), seq)])

    def sum_out(k, j, q, ref):
        peer = device(z, lax.rem(x + j, xs), lax.rem(y + q, sides), c)
        at = place(k, j, q)
        arrived[SUM_P, k, j, q] = send(ref, r.plane_sums.at[at], SUM_P, at, peer)

    def add_dense(k):
        for q in range(sides):
            arrived[HIDDEN_C, k, q].wait_recv()
        if k == 0:
            got.ddv.wait()
        dense = sum(
            jnp.dot(
                r.dhid[k, t], r.ddv[t * dff : (t + 1) * dff, :], preferred_element_type=F32
            )
            for t in range(tpn)
        )
        r.keep[k] = r.keep[k] + jax.nn.sigmoid(r.mix_v[...]) * dense
        for j in range(1, xs):
            slot = k * sides
            rows_at = span(lax.rem(x + j, xs), seq)
            r.ysend[slot, rows_at, :] = r.keep[k, rows_at, :].astype(BF16)
            sum_out(k, j, 0, r.ysend.at[slot, rows_at])

    def from_sums(k):
        value = r.keep[k, span(x, seq), :]
        for j, q in offsets[1:]:
            arrived[SUM_P, k, j, q].wait_recv()
            value = value + r.plane_sums[place(k, j, q)].astype(F32)
        if k == 0:
            r.resid[...] = r.resid[...] + value
        else:
            r.zsend[k] = value.astype(BF16)
            send(r.zsend.at[k], r.zrecv.at[z], SUM_Z, k, device(zat(k), x, y, c), z)

    def write_state(k):
        lax.fori_loop(0, groups, write_group, 0)

    kinds = (
        from_z,
        from_plane,
        first_half,
        second_half,
        down,
        dense_hidden,
        from_twin,
        hidden_on,
        add_dense,
        from_sums,
        scale_out,
        write_state,
    )
    for kind, k in schedule(zs):
        step = kinds[kind]
        step(k)

    final = r.resid[...]
    for k in range(1, zs):
        landed(SUM_Z, zat(k), r.zrecv.at[zat(k)])
        final = final + r.zrecv[zat(k)].astype(F32)
    r.out[...] = final.astype(BF16)

    for copy in waiting:
        copy.wait_send()


def place_kernel(held, held_state, out, new_state, sems):
    parts = [pl.ds(g * ROWS, ROWS) for g in range(held_state.shape[0] // ROWS)]
    moves = [(held_state.at[p], new_state.at[p]) for p in parts] + [(held, out)]
    copies = [pltpu.make_async_copy(*move, sems.at[k]) for k, move in enumerate(moves)]
    for copy in copies:
        copy.start()
    for copy in copies:
        copy.wait()


def local(
    tokens,
    state,
    norm_gain,
    w_query,
    w_forget,
    w_input,
    w_outgate,
    lower_bound,
    head_gain,
    w_output,
    ffn_gain,
    route_ids,
    route_weight,
    expert_gate,
    expert_up,
    expert_down,
    shared_gate,
    shared_up,
    shared_down,
    dense_gate,
    dense_up,
    dense_down,
    dense_mix,
):
    n = lax.axis_size("ep")
    tpn = lax.axis_size("tp")
    sides = tpn // CORES
    zs = n // sides
    seq, width = tokens.shape
    depth, mixw = w_query.shape
    heads, hd = state.shape[1:3]
    cols = width // tpn
    half = sides * cols
    exp_local, _, ff = expert_gate.shape
    sff = shared_gate.shape[1]
    dff = dense_gate.shape[1] // tpn
    lanes = ceil_to(seq, LANES)
    rrows = ceil_to(exp_local, ROWS)
    groups = seq // ROWS
    move = dff % LANES == 0
    sds = jax.ShapeDtypeStruct
    VM, ANY = pltpu.VMEM, pl.ANY

    ins = dict(
        tokens=tokens,
        state=state,
        gain1=norm_gain[None, :],
        wq=w_query,
        wf=w_forget,
        wi=w_input,
        wo=w_outgate,
        lb=lower_bound[None, :],
        hg=head_gain[None, :],
        wout=w_output,
        gain2=ffn_gain[None, :],
        ids=route_ids.T,
        weights=route_weight.T,
        eg=expert_gate,
        eu=expert_up,
        ed=expert_down,
        sg=shared_gate,
        su=shared_up,
        sd=shared_down,
        mix=dense_mix[None, :],
        ddown=dense_down,
    )
    if move:
        ins.update(dgate=dense_gate, dup=dense_up)
    else:
        gate_w, up_w = [
            lax.all_to_all(w, "tp", split_axis=1, concat_axis=0, tiled=True)
            for w in (dense_gate, dense_up)
        ]
        ins.update(gatew=gate_w, upw=up_w)
    outs = dict(out=sds((seq, cols), BF16), new_state=sds(state.shape, F32))
    hops = zs * sides * sides
    size = sides * seq
    scratch = dict(
        tokens_v=VM((seq, width), BF16),
        gain1_v=VM((1, width), F32),
        gain2_v=VM((1, width), F32),
        lb_v=VM((1, mixw), F32),
        hg_v=VM((1, mixw), F32),
        mix_v=VM((1, cols), F32),
        ids_v=VM(route_ids.shape[::-1], jnp.int32),
        weights_v=VM(route_weight.shape[::-1], F32),
        wout_v=VM((mixw, width), BF16),
        nsend=VM((zs * seq, sides * depth), BF16),
        ncol=VM((zs * seq, sides * depth), BF16),
        wbuf=VM((4, sides * depth, mixw), BF16),
        psend=VM((4, zs * seq, mixw), BF16),
        precv=VM((4, zs * seq, mixw), BF16),
        dturn=VM((groups, mixw, ROWS), F32),
        qturn=VM((groups, mixw, ROWS), F32),
        vals=VM((seq, mixw), F32),
        read=VM((seq, mixw), F32),
        rsend=VM((n, rrows, lanes), F32),
        rrecv=VM((n, rrows, lanes), F32),
        hsend=VM((tpn, seq, cols), BF16),
        hrecv=VM((tpn, seq, cols), BF16),
        resid=VM((seq, cols), F32),
        rows=VM((CORES, n * seq, half), BF16),
        sqs=VM((ROWS, lanes), F32),
        sqr=VM((tpn, ROWS, lanes), F32),
        scr=VM((n, ROWS, lanes), F32),
        egv=VM((CORES, exp_local, half, ff), BF16),
        euv=VM((CORES, exp_local, half, ff), BF16),
        edv=VM((exp_local * ff, width), BF16),
        sgv=VM((CORES, half, sff), BF16),
        suv=VM((CORES, half, sff), BF16),
        sdv=VM((sff, width), BF16),
        dgv=VM((CORES, half, dff), BF16),
        duv=VM((CORES, half, dff), BF16),
        ddv=VM(dense_down.shape, BF16),
        acc=VM((2 * exp_local, zs, size, ff), F32),
        hid=VM((zs, size, exp_local * ff), BF16),
        dhid=VM((zs, tpn, size, dff), BF16),
        wide=VM((size, cols), F32),
        part=VM((zs * sides, size, cols), BF16),
        crecv=VM((zs * sides, size, cols), BF16),
        ysend=VM((zs * sides, size, cols), BF16),
        plane_sums=VM((hops, seq, cols), BF16),
        keep=VM((zs, size, cols), F32),
        zsend=VM((zs, seq, cols), BF16),
        zrecv=VM((zs, seq, cols), BF16),
        shared=VM((tpn, seq, cols), F32),
        local=pltpu.SemaphoreType.DMA((64 + groups + 8 * exp_local * tpn,)),
    )
    counts = {
        WEIGHT: 4 * sides,
        NORMED: zs,
        MOVE: 2 * tpn * PIECES,
        ROUTE: n,
        HIDDEN_Y: zs * sides,
        HIDDEN_C: zs * sides,
        PROJ: 4 * zs,
        HEAD: tpn,
        GATHER_Z: zs,
        GATHER_P: hops,
        GATHER_C: hops,
        SQUARE: tpn,
        SCALE: n,
        SUM_C: zs * sides,
        SUM_P: hops,
        SUM_Z: zs,
    }
    names = [*ins, *outs, *scratch]
    sems = [pltpu.SemaphoreType.DMA((counts[k],)) for k in range(len(counts)) for _ in range(2)]
    held = pl.pallas_call(
        functools.partial(layer_kernel, n, tpn, move, names),
        out_shape=tuple(VM(out.shape, out.dtype) for out in outs.values()),
        in_specs=[pl.BlockSpec(memory_space=ANY) for _ in ins],
        out_specs=(pl.BlockSpec(memory_space=VM),) * 2,
        scratch_shapes=list(scratch.values()) + sems,
        compiler_params=pltpu.CompilerParams(
            collective_id=0, has_side_effects=True, vmem_limit_bytes=VMEM_BYTES
        ),
    )(*ins.values())
    return pl.pallas_call(
        place_kernel,
        out_shape=tuple(outs.values()),
        in_specs=[pl.BlockSpec(memory_space=VM)] * 2,
        out_specs=(pl.BlockSpec(memory_space=ANY),) * 2,
        scratch_shapes=[pltpu.SemaphoreType.DMA((groups + 1,))],
        compiler_params=pltpu.CompilerParams(vmem_limit_bytes=PLACE_BYTES),
    )(*[pltpu.with_memory_space_constraint(a, VM) for a in held])


def solution(mesh):
    placed = (
        P("ep", None),
        P("ep", "tp", None, None),
        P(),
        P("ep", "tp"),
        P("ep", "tp"),
        P("ep", "tp"),
        P("ep", "tp"),
        P("tp"),
        P("tp"),
        P("tp", None),
        P(),
        P("ep", None),
        P("ep", None),
        P("ep", None, "tp"),
        P("ep", None, "tp"),
        P("ep", "tp", None),
        P(None, "tp"),
        P(None, "tp"),
        P("tp", None),
        P("tp", "ep"),
        P("tp", "ep"),
        P("ep", "tp"),
        P("tp"),
    )
    return jax.shard_map(
        local,
        mesh=mesh,
        in_specs=placed,
        out_specs=(P("ep", "tp"), P("ep", "tp", None, None)),
        check_vma=False,
    )
```
